32 devices in a mesh: sp: 8 (over z, y), tp: 4 (over x, core).
Axes of the slice: x: 2, y: 2, z: 4, core: 2. Of those that a mesh axis runs over, the one named last changes fastest.
Arguments:
- resid: bfloat16 [8192, 2048], P(('sp', 'tp')), may hold values from -6 to 6
- query_nope: bfloat16 [8192, 2048], P('sp', 'tp'), may hold values from -18 to 18
- query_rope: bfloat16 [8192, 1024], P('sp', 'tp'), may hold values from -300 to 300
- latent: bfloat16 [8192, 256], P('sp'), may hold values from -6 to 6
- key_rope: bfloat16 [8192, 64], P('sp'), may hold values from -6 to 6
- latent_gain: float32 [256], replicated, may hold values from 0.1 to 1.9
- w_key: bfloat16 [256, 2048], P(None, 'tp'), may hold values from -0.375 to 0.375
- w_value: bfloat16 [256, 2048], P(None, 'tp'), may hold values from -0.375 to 0.375
- w_out: bfloat16 [2048, 2048], P('tp'), may hold values from -0.125 to 0.125
- mix_gain: float32 [2048], replicated, may hold values from 0.1 to 1.9
- w_gate: bfloat16 [2048, 5632], P('sp', 'tp'), may hold values from -0.125 to 0.125
- w_up: bfloat16 [2048, 5632], P('sp', 'tp'), may hold values from -0.125 to 0.125
- w_down: bfloat16 [2048, 5632], P('sp', 'tp'), may hold values from -0.078125 to 0.078125
Outputs:
- layer_out: bfloat16 [8192, 2048], P(('sp', 'tp'))
The draws below stay inside these ranges and needn't reach their ends.
All inputs are finite; a program needn't handle non-finite values.
Results may differ from the reference program's by a relative error of at most 0.0095.
Values may be sent and summed in bfloat16 or wider, within the bound.
A program may use at most 128 MiB of HBM per device.

```python
import jax
import jax.numpy as jnp
from jax import lax

D = 2048
HEADS = 16
NOPE = 128
ROPE = 64
VDIM = 128
RANK = 256
FF = 5632
TOK_DEV = 1024
TOKENS = 8192
N_SP = 8
N_TP = 4


def rope_pair(key):
    base_key = jax.random.fold_in(key, 11)
    key_one, key_two = jax.random.split(base_key, 2)
    key_part = jax.random.truncated_normal(key_one, -5.0, 5.0, (TOKENS, ROPE), jnp.float32)
    query_part = 3.0 * jax.random.truncated_normal(key_two, -5.0, 5.0, (TOKENS, HEADS * ROPE), jnp.float32)
    return (key_part, query_part)


def draw_query_rope(key, part):
    return rope_pair(key)[1].astype(jnp.bfloat16)


def draw_key_rope(key, part):
    return rope_pair(key)[0].astype(jnp.bfloat16)


def block_levels(key, dims, cuts, least, top_value):
    def one(position, blocks):
        heights = jax.random.uniform(jax.random.fold_in(jax.random.fold_in(key, 6), position), (blocks,), jnp.float32, least / len(cuts), top_value / len(cuts))
        return jnp.repeat(jnp.exp(heights), dims[position] // blocks).reshape((-1,) + (1,) * (len(dims) - position - 1))

    factor_of = one(*cuts[0])
    for cut in cuts[1:]:
        factor_of = factor_of * one(*cut)
    return factor_of


def bell_draw(stream_key, dims, spread, reach, cuts=(), held_as=jnp.bfloat16):
    loudness = block_levels(stream_key, dims, cuts, -0.22, 0.18) if cuts else 1.0
    result = jax.random.normal(stream_key, dims, jnp.float32) * spread * loudness
    return jnp.minimum(jnp.maximum(result, -reach), reach).astype(held_as)


def setup_inputs(seed: int = 0) -> dict:
    splits = jax.random.split(jax.random.key(seed), 14)
    resid = bell_draw(splits[0], (TOKENS, D), 1.0, 6.0, ((0, 32),))
    query_nope = bell_draw(splits[1], (TOKENS, HEADS * NOPE), 3.0, 18.0, ((0, 8), (1, 4)))
    query_rope = draw_query_rope(jax.random.fold_in(splits[13], 71), 0)
    latent = bell_draw(splits[3], (TOKENS, RANK), 1.0, 6.0, ((0, 8),))
    key_rope = draw_key_rope(jax.random.fold_in(splits[13], 71), 0)
    latent_gain = jnp.clip(1.0 + 0.18 * jax.random.normal(splits[5], (RANK,), jnp.float32), 0.1, 1.9)
    w_key = bell_draw(splits[6], (RANK, HEADS * NOPE), RANK ** -0.5, 0.375, ((1, 4),))
    w_value = bell_draw(splits[7], (RANK, HEADS * VDIM), RANK ** -0.5, 0.375, ((1, 4),))
    w_out = bell_draw(splits[8], (HEADS * VDIM, D), (HEADS * VDIM) ** -0.5, 0.125, ((0, 4),))
    mix_gain = jnp.clip(1.0 + 0.18 * jax.random.normal(splits[9], (D,), jnp.float32), 0.1, 1.9)
    w_gate = bell_draw(splits[10], (D, FF), D ** -0.5, 0.125, ((0, 8), (1, 4)))
    w_up = bell_draw(splits[11], (D, FF), D ** -0.5, 0.125, ((0, 8), (1, 4)))
    w_down = bell_draw(splits[12], (D, FF), FF ** -0.5, 0.078125, ((0, 8), (1, 4)))
    return {"resid": resid, "query_nope": query_nope, "query_rope": query_rope, "latent": latent, "key_rope": key_rope, "latent_gain": latent_gain, "w_key": w_key, "w_value": w_value, "w_out": w_out, "mix_gain": mix_gain, "w_gate": w_gate, "w_up": w_up, "w_down": w_down}


norm_eps = 1e-06
masked_score = -1e+30
theta_base = 10000.0

def rotate(values_in, angle):
    half_width = values_in.shape[-1] // 2
    front_half = values_in[..., :half_width]
    back_half = values_in[..., half_width:]
    cosine = jnp.cos(angle)
    sine_part = jnp.sin(angle)
    return jnp.concatenate([front_half * cosine - back_half * sine_part, back_half * cosine + front_half * sine_part], axis=-1)

def angles(positions, full_width):
    half_width = full_width // 2
    frequency = theta_base ** (-2.0 * jnp.arange(half_width).astype(jnp.float32) / full_width)
    return positions[:, None] * frequency[None, :]

def rms_scale(values_in, gain):
    return values_in * lax.rsqrt(lax.optimization_barrier(jnp.mean(values_in * values_in, axis=-1, keepdims=True)) + norm_eps) * gain

def reference(resid, query_nope, query_rope, latent, key_rope, latent_gain, w_key, w_value, w_out, mix_gain, w_gate, w_up, w_down):
    positions = jnp.arange(TOKENS).astype(jnp.float32)
    angle = angles(positions, ROPE)
    latent_normed = rms_scale(latent.astype(jnp.float32), latent_gain).astype(jnp.bfloat16)
    head_keys = jnp.dot(latent_normed, w_key, preferred_element_type=jnp.float32).astype(jnp.bfloat16)
    head_values = jnp.dot(latent_normed, w_value, preferred_element_type=jnp.float32).astype(jnp.bfloat16)
    key_rotated = rotate(key_rope.astype(jnp.float32), angle).astype(jnp.bfloat16)
    query_rotated = rotate(query_rope.astype(jnp.float32).reshape(TOKENS, HEADS, ROPE), angle[:, None, :]).astype(jnp.bfloat16)
    by_head_nope = jnp.transpose(query_nope.reshape(TOKENS, HEADS, NOPE), (1, 0, 2))
    by_head_rope = jnp.transpose(query_rotated, (1, 0, 2))
    by_head_keys = jnp.transpose(head_keys.reshape(TOKENS, HEADS, NOPE), (1, 0, 2))
    by_head_values = jnp.transpose(head_values.reshape(TOKENS, HEADS, VDIM), (1, 0, 2))
    score_scale = (NOPE + ROPE) ** (-0.5)
    key_positions = jnp.arange(TOKENS).astype(jnp.int32)

    def one_head(operands):
        nope_q, rope_q, keys_h, values_h = operands

        def one_block(block_index):
            first_row = block_index * TOK_DEV
            query_part = lax.dynamic_slice_in_dim(nope_q, first_row, TOK_DEV, 0)
            rope_part = lax.dynamic_slice_in_dim(rope_q, first_row, TOK_DEV, 0)
            scores = jnp.dot(query_part, keys_h.T, preferred_element_type=jnp.float32)
            scores = (scores + jnp.dot(rope_part, key_rotated.T, preferred_element_type=jnp.float32)) * score_scale
            query_rows = first_row + jnp.arange(TOK_DEV).astype(jnp.int32)
            causal = key_positions[None, :] <= query_rows[:, None]
            scores = jnp.where(causal, scores, masked_score)
            row_max = lax.optimization_barrier(jnp.max(scores, axis=-1, keepdims=True))
            weights = jnp.where(causal, jnp.exp(scores - row_max), 0.0)
            weight_sum = lax.optimization_barrier(jnp.sum(weights, axis=-1, keepdims=True))
            mixed = jnp.dot(weights.astype(jnp.bfloat16), values_h, preferred_element_type=jnp.float32)
            return (mixed / weight_sum).astype(jnp.bfloat16)
        return lax.map(one_block, jnp.arange(N_SP).astype(jnp.int32))
    head_out = lax.map(one_head, (by_head_nope, by_head_rope, by_head_keys, by_head_values))
    head_out = head_out.reshape(HEADS, TOKENS, VDIM)
    group_heads = HEADS // N_TP
    out_heads = w_out.reshape(HEADS, VDIM, D)
    attention_proj = jnp.zeros((TOKENS, D), jnp.float32)
    for group_index in range(N_TP):
        picked = slice(group_index * group_heads, (group_index + 1) * group_heads)
        partial_sum = jnp.einsum('htv,hvd->td', head_out[picked].astype(jnp.float32), out_heads[picked].astype(jnp.float32))
        attention_proj = attention_proj + lax.optimization_barrier(partial_sum.astype(jnp.bfloat16)).astype(jnp.float32)
    stream = resid.astype(jnp.float32) + attention_proj
    normed = rms_scale(stream, mix_gain).astype(jnp.bfloat16)
    group_units = FF // N_TP
    mixer_out = jnp.zeros((TOKENS, D), jnp.float32)
    for group_index in range(N_TP):
        columns = slice(group_index * group_units, (group_index + 1) * group_units)
        gate_value = jnp.dot(normed, w_gate[:, columns], preferred_element_type=jnp.float32)
        upward = jnp.dot(normed, w_up[:, columns], preferred_element_type=jnp.float32)
        hidden = (jax.nn.silu(gate_value) * upward).astype(jnp.bfloat16)
        partial_sum = jnp.dot(hidden, w_down[:, columns].T, preferred_element_type=jnp.float32)
        mixer_out = mixer_out + lax.optimization_barrier(partial_sum.astype(jnp.bfloat16)).astype(jnp.float32)
    return (stream + 0.5 * mixer_out).astype(jnp.bfloat16)
```

```python
import functools

import jax
import jax.numpy as jnp
from jax import lax
from jax.experimental import pallas as pl
from jax.experimental.pallas import tpu as pltpu
from jax.sharding import PartitionSpec as P

NOPE = 128
ROPE = 64
VDIM = 128
LANES = 128
ONES = 16

norm_eps = 1e-06
masked_score = -1e30
theta_base = 10000.0
LOG2E = 1.4426950408889634
COLS = (((1,), (1,)), ((), ()))
MIB = 1024 * 1024
MESH = pl.DeviceIdType.MESH
F32 = jnp.float32
BF16 = jnp.bfloat16


def ring_order(count):
    narrow = 1
    while (2 * narrow) ** 2 <= count and count % (2 * narrow) == 0:
        narrow *= 2
    long = count // narrow
    if narrow == 1 or long % 2:
        return list(range(count))
    order = []
    for row in range(long):
        columns = range(1, narrow) if row % 2 == 0 else range(narrow - 1, 0, -1)
        order += [row * narrow + column for column in columns]
    return order + [row * narrow for row in reversed(range(long))]


def divisor(size, choices):
    return next(choice for choice in choices if size % choice == 0)


def pick(table, index):
    found = jnp.int32(0)
    for i, value in enumerate(table):
        found = jnp.where(index == i, jnp.int32(value), found)
    return found


def remote(src, dst, send, recv, where):
    return pltpu.make_async_remote_copy(
        src_ref=src, dst_ref=dst, send_sem=send, recv_sem=recv, device_id=where, device_id_type=MESH
    )


def layer_kernel(
    n_sp,
    n_tp,
    tile,
    chunk,
    resid_ref,
    qn_ref,
    qr_ref,
    lat_ref,
    kr_ref,
    freq_ref,
    gain_ref,
    mix_ref,
    wb_ref,
    wo_ref,
    wg_ref,
    wu_ref,
    wd_ref,
    o_ref,
    gate_all,
    up_all,
    down_all,
    wo_all,
    lat_all,
    q_s,
    k_s,
    v_s,
    m_s,
    acc_s,
    s_s,
    mx_s,
    ho_s,
    tr_s,
    wo_s,
    x_s,
    stream_s,
    gate_s,
    up_s,
    hid_s,
    g_buf,
    u_buf,
    keep_s,
    pair_out,
    pair_in,
    cross_out,
    cross_in,
    lat_ring,
    lat_pair,
    lat_side,
    lat_relay,
    wo_sem,
    ring_sem,
    down_sem,
    trade_sem,
    x_sem,
    pair_sem,
    cross_sem,
    local_sem,
):
    me = lax.axis_index("sp")
    mine = lax.axis_index("tp")
    rows = qr_ref.shape[0]
    heads = wb_ref.shape[0]
    rank = wb_ref.shape[1]
    depth = resid_ref.shape[1]
    share = rows // n_tp
    part = wg_ref.shape[0]
    half = part // 2
    n_x = n_tp // 2
    x_at, core = mine // 2, lax.rem(mine, 2)
    partner = mine + 1 - 2 * core
    forward = n_sp // 2
    backward = n_sp - 1 - forward
    events = 2 * (n_sp - 1)

    order = ring_order(n_sp)
    place = pick([order.index(i) for i in range(n_sp)], me)

    def at_place(offset):
        return pick(order, lax.rem(place + offset + 2 * n_sp, n_sp))

    right, left = at_place(1), at_place(-1)
    to_right, to_left = {"sp": right, "tp": mine}, {"sp": left, "tp": mine}
    to_partner = {"sp": me, "tp": partner}

    def side(d):
        return lax.rem(x_at + d, n_x) * 2 + core

    def to_side(d):
        return {"sp": me, "tp": side(d)}

    def from_side(d):
        return lax.rem(x_at - d + n_x, n_x) * 2 + core

    barrier = pltpu.get_barrier_semaphore()
    pl.semaphore_signal(barrier, inc=1, device_id=to_right, device_id_type=MESH)
    pl.semaphore_signal(barrier, inc=1, device_id=to_left, device_id_type=MESH)
    for d in range(1, n_tp):
        peer = {"sp": me, "tp": lax.rem(mine + d, n_tp)}
        pl.semaphore_signal(barrier, inc=1, device_id=peer, device_id_type=MESH)
    pl.semaphore_wait(barrier, n_tp + 1)

    def piece(ref, i):
        return ref.at[pl.ds(pl.multiple_of(i * half, half), half), :]

    def ring_copies(e, first=False):
        hop, i = e // 2 + 1, lax.rem(e, 2)
        behind, beyond = at_place(1 - hop), at_place(hop - 1)
        return (
            remote(
                piece(wg_ref if first else gate_all.at[behind], i),
                piece(gate_all.at[behind], i),
                ring_sem.at[0, e],
                ring_sem.at[1, e],
                to_right,
            ),
            remote(
                piece(wu_ref if first else up_all.at[beyond], i),
                piece(up_all.at[beyond], i),
                ring_sem.at[2, e],
                ring_sem.at[3, e],
                to_left,
            ),
        )

    def down_ahead(hop, first=False):
        owner = at_place(1 - hop)
        return remote(
            wd_ref if first else down_all.at[owner],
            down_all.at[owner],
            down_sem.at[0, hop],
            down_sem.at[1, hop],
            to_right,
        )

    def down_back(hop, first=False):
        owner = at_place(hop - 1)
        return remote(
            wd_ref if first else down_all.at[owner],
            down_all.at[owner],
            down_sem.at[2, hop],
            down_sem.at[3, hop],
            to_left,
        )

    def ring_event(e):
        for copy in ring_copies(e):
            copy.wait_recv()

        @pl.when(e + 2 < events)
        def _():
            for copy in ring_copies(e + 2):
                copy.start()

        @pl.when(e == events - 3)
        def _():
            down_ahead(1, True).start()
            down_back(1, True).start()

    def quarter(owner, t):
        return lat_all.at[owner, pl.ds(pl.multiple_of(t * share, share), share), :]

    def lat_hop(hop, way):
        owner = at_place(jnp.where(way == 0, 1 - hop, hop - 1))
        where = {"sp": jnp.where(way == 0, right, left), "tp": mine}
        return remote(
            quarter(owner, mine),
            quarter(owner, mine),
            lat_ring.at[0, way, hop],
            lat_ring.at[1, way, hop],
            where,
        )

    def lat_owner(hop, way):
        return at_place(jnp.where(way == 0, -hop, hop))

    def lat_pair_copy(hop, way, t):
        owner = lat_owner(hop, way)
        return remote(
            quarter(owner, t),
            quarter(owner, t),
            lat_pair.at[0, way, hop],
            lat_pair.at[1, way, hop],
            to_partner,
        )

    def lat_side_copy(hop, way, d, t):
        owner = lat_owner(hop, way)
        return remote(
            quarter(owner, t),
            quarter(owner, t),
            lat_side.at[0, way, hop, d],
            lat_side.at[1, way, hop, d],
            to_side(d),
        )

    def lat_relay_copy(hop, way, d, t):
        owner = lat_owner(hop, way)
        return remote(
            quarter(owner, t),
            quarter(owner, t),
            lat_relay.at[0, way, hop, d],
            lat_relay.at[1, way, hop, d],
            to_partner,
        )

    def ways(hop):
        return jnp.where(hop <= backward, 2, 1)

    def lat_forward(hop):
        def one(way, carry):
            lat_hop(hop, way).wait_recv()

            @pl.when(hop + 1 <= jnp.where(way == 0, forward, backward))
            def _():
                lat_hop(hop + 1, way).start()

            for d in range(1, n_x):
                lat_side_copy(hop, way, d, mine).start()
            lat_pair_copy(hop, way, mine).start()
            return carry

        lax.fori_loop(0, ways(hop), one, 0)

    def lat_pass(hop):
        def one(way, carry):
            for d in range(1, n_x):
                lat_side_copy(hop, way, d, from_side(d)).wait_recv()
                lat_relay_copy(hop, way, d, from_side(d)).start()
            return carry

        lax.fori_loop(0, ways(hop), one, 0)

    def lat_ready(hop, way):
        lat_pair_copy(hop, way, partner).wait_recv()
        for d in range(1, n_x):
            lat_relay_copy(hop, way, d, from_side(d) + 1 - 2 * core).wait_recv()

    def wo_copy(kind, d, t, src=None):
        where = to_partner if kind != 1 else to_side(d)
        return remote(
            wo_all.at[t] if src is None else src,
            wo_all.at[t],
            wo_sem.at[0, kind, d],
            wo_sem.at[1, kind, d],
            where,
        )

    def rotated(values, span):
        first = first_row + span
        position = (first + lax.broadcasted_iota(jnp.int32, values.shape, 0)).astype(F32)
        angle = position * freq_ref[...]
        front = lax.rem(lax.broadcasted_iota(jnp.int32, values.shape, 1), ROPE) < ROPE // 2
        return angle, front

    def turn(values, cosine, sine, front):
        other = jnp.where(
            front,
            pltpu.roll(values, LANES - ROPE // 2, 1),
            pltpu.roll(values, ROPE // 2, 1),
        )
        return values * cosine + other * sine

    first_row = me * rows

    def prepare(i, carry):
        start = pl.multiple_of(i * share, share)
        span = pl.ds(start, share)
        key = kr_ref[span, :].astype(F32)
        key = jnp.concatenate([key, key], axis=1)
        angle, front = rotated(key, start)
        cosine = jnp.cos(angle)
        sine = jnp.sin(angle)
        sine = jnp.where(front, -sine, sine)
        lat_all[me, span, rank:] = turn(key, cosine, sine, front).astype(BF16)
        latent = lat_ref[span, :].astype(F32)
        power = jnp.mean(latent * latent, axis=1, keepdims=True)
        latent = latent * lax.rsqrt(power + norm_eps) * gain_ref[...]
        lat_all[me, span, :rank] = latent.astype(BF16)
        for j in range(heads // 2):
            pair = qr_ref[span, j * LANES : (j + 1) * LANES].astype(F32)
            pair = turn(pair, cosine, sine, front)
            q_s[2 * j, span, NOPE:] = pair.astype(BF16)
            q_s[2 * j + 1, span, NOPE:] = pltpu.roll(pair, ROPE, 1).astype(BF16)
        for h in range(heads):
            q_s[h, span, :NOPE] = qn_ref[span, h * NOPE : (h + 1) * NOPE]
        return carry

    lax.fori_loop(0, n_tp, prepare, 0)
    lat_hop(1, jnp.int32(0)).start()
    if backward:
        lat_hop(1, jnp.int32(1)).start()
    for e in range(2):
        for copy in ring_copies(jnp.int32(e), True):
            copy.start()
    wo_copy(0, 0, mine, wo_ref).start()
    for d in range(1, n_x):
        wo_copy(1, d, mine, wo_ref).start()
    wo_mine = pltpu.make_async_copy(wo_ref, wo_all.at[mine], local_sem.at[0, 0])
    wo_mine.start()

    tiles = rows // tile
    chunks = rows // chunk
    total = heads * tiles
    scale = (NOPE + ROPE) ** (-0.5) * LOG2E

    m_s[...] = jnp.full_like(m_s, masked_score)
    acc_s[...] = jnp.zeros_like(acc_s)
    for h in range(heads):
        v_s[h, VDIM:, :] = jnp.ones((ONES, rows), BF16)

    def project(owner):
        def one(h, carry):
            both = jnp.dot(
                lat_all[owner, :, :rank], wb_ref[h], preferred_element_type=F32
            ).astype(BF16)
            k_s[h, :, :NOPE] = both[:, :NOPE]
            k_s[h, :, NOPE:] = lat_all[owner, :, rank:]
            v_s[h, :VDIM, :] = both[:, NOPE:].T
            return carry

        lax.fori_loop(0, heads, one, 0)

    def span_of(t):
        return pl.ds(t * tile if isinstance(t, int) else pl.multiple_of(t * tile, tile), tile)

    def score(h, t, c, slot, top, diagonal):
        keys = slice(c * chunk, (c + 1) * chunk)
        scores = scale * lax.dot_general(
            k_s[h, keys, : NOPE + ROPE],
            q_s[h, span_of(t), : NOPE + ROPE],
            COLS,
            preferred_element_type=F32,
        )
        if diagonal:
            row = t * tile + lax.broadcasted_iota(jnp.int32, scores.shape, 1)
            col = c * chunk + lax.broadcasted_iota(jnp.int32, scores.shape, 0)
            scores = jnp.where(col <= row, scores, masked_score)
        s_s[slot, keys, :] = scores
        peak = jnp.max(scores.reshape(chunk // 8, 8, tile), axis=0)
        return peak if top is None else jnp.maximum(top, peak)

    def advance(h, t, peak):
        old = m_s[h, :, span_of(t)]
        top = jnp.maximum(old, jnp.max(peak, axis=0, keepdims=True))
        m_s[h, :, span_of(t)] = top
        return top[:1], jnp.exp2(old - top)[:1]

    def fold(h, c, slot, top, mixed):
        keys = slice(c * chunk, (c + 1) * chunk)
        weights = jnp.exp2(s_s[slot, keys, :] - top).astype(BF16)
        term = jnp.dot(v_s[h, :, keys], weights, preferred_element_type=F32)
        return term if mixed is None else mixed + term

    def finish(h, t, factor, mixed):
        acc_s[h, :, span_of(t)] = acc_s[h, :, span_of(t)] * factor + mixed

    project(me)

    def own_head(h, carry):
        for t in range(tiles):
            peak = mixed = None
            limit = -(-(t + 1) * tile // chunk)
            for c in range(limit):
                peak = score(h, t, c, t % 2, peak, (c + 1) * chunk > t * tile)
            top, factor = advance(h, t, peak)
            for c in range(limit):
                mixed = fold(h, c, t % 2, top, mixed)
            finish(h, t, factor, mixed)
        return carry

    lax.fori_loop(0, heads, own_head, 0)

    def attend(owner):
        project(owner)
        peak = None
        for c in range(chunks):
            peak = score(0, 0, c, 0, peak, False)
        mx_s[0] = peak

        def one(i, slot):
            h, t = i // tiles, lax.rem(i, tiles)
            later = jnp.minimum(i + 1, total - 1)
            next_h, next_t = later // tiles, lax.rem(later, tiles)
            top, factor = advance(h, t, mx_s[slot])
            peak = mixed = None
            for c in range(chunks):
                peak = score(next_h, next_t, c, 1 - slot, peak, False)
                mixed = fold(h, c, slot, top, mixed)
            mx_s[1 - slot] = peak
            finish(h, t, factor, mixed)

        def two(i, carry):
            one(2 * i, 0)
            one(2 * i + 1, 1)
            return carry

        lax.fori_loop(0, total // 2, two, 0)

    lat_forward(jnp.int32(1))
    lat_pass(jnp.int32(1))

    def block(i, carry):
        hop = i // 2 + 1
        way = lax.rem(i, 2)

        @pl.when(way < ways(hop))
        def _():
            lat_ready(hop, way)
            owner = lat_owner(hop, way)

            @pl.when(owner < me)
            def _():
                attend(owner)

        @pl.when(jnp.logical_and(way == 0, hop < forward))
        def _():
            lat_forward(hop + 1)

        @pl.when(jnp.logical_and(way == 1, hop < forward))
        def _():
            lat_pass(hop + 1)

        ring_event(i)
        return carry

    lax.fori_loop(0, 2 * forward, block, 0)
    serviced = 2 * forward

    def finish_head(h):
        done = acc_s[h]
        out = (done[:VDIM] / done[VDIM : VDIM + 1]).T.astype(BF16)
        for r in range(n_tp):
            ho_s[r, :, h * VDIM : (h + 1) * VDIM] = out[r * share : (r + 1) * share]

    for h in range(heads):
        finish_head(h)
    tr_s[mine] = ho_s[mine]

    def trade(d):
        target = lax.rem(mine + d, n_tp)
        return remote(
            ho_s.at[target],
            tr_s.at[mine],
            trade_sem.at[0, d],
            trade_sem.at[1, d],
            {"sp": me, "tp": target},
        )

    def traded(d):
        source = lax.rem(mine - d + n_tp, n_tp)
        return remote(
            ho_s.at[source],
            tr_s.at[source],
            trade_sem.at[0, d],
            trade_sem.at[1, d],
            {"sp": me, "tp": source},
        )

    for d in range(1, n_tp):
        trade(d).start()
    for d in range(1, n_x):
        wo_copy(1, d, from_side(d)).wait_recv()
        wo_copy(2, d, from_side(d)).start()
    wo_copy(0, 0, partner).wait_recv()
    for d in range(1, n_x):
        wo_copy(2, d, from_side(d) + 1 - 2 * core).wait_recv()
    wo_mine.wait()

    wide = wo_s.shape[3]
    columns = depth // wide

    def wo_load(j):
        return pltpu.make_async_copy(
            wo_all.at[:, :, j * wide : (j + 1) * wide], wo_s.at[j % 2], local_sem.at[1, j % 2]
        )

    wo_load(0).start()
    for d in range(1, n_tp):
        traded(d).wait_recv()
    for j in range(columns):
        wo_load(j).wait()
        if j + 1 < columns:
            wo_load(j + 1).start()
        proj = resid_ref[:, j * wide : (j + 1) * wide].astype(F32)
        for g in range(n_tp):
            proj += jnp.dot(tr_s[g], wo_s[j % 2, g], preferred_element_type=F32)
        stream_s[:, j * wide : (j + 1) * wide] = proj

    strip = divisor(share, (64, 32, 16, 8))

    def normalise(i, carry):
        span = pl.ds(pl.multiple_of(i * strip, strip), strip)
        stream = stream_s[span, :]
        power = jnp.mean(stream * stream, axis=1, keepdims=True)
        x_s[mine, span, :] = (stream * lax.rsqrt(power + norm_eps) * mix_ref[...]).astype(BF16)
        return carry

    lax.fori_loop(0, share // strip, normalise, 0)

    def x_copy(kind, d, t):
        where = to_partner if kind != 1 else to_side(d)
        return remote(x_s.at[t], x_s.at[t], x_sem.at[0, kind, d], x_sem.at[1, kind, d], where)

    for d in range(1, n_x):
        x_copy(1, d, mine).start()
    x_copy(0, 0, mine).start()
    for _ in range(2):
        ring_event(jnp.int32(serviced))
        serviced += 1
    for d in range(1, n_x):
        x_copy(1, d, from_side(d)).wait_recv()
        x_copy(2, d, from_side(d)).start()
    for _ in range(2):
        ring_event(jnp.int32(serviced))
        serviced += 1
    x_copy(0, 0, partner).wait_recv()
    for d in range(1, n_x):
        x_copy(2, d, from_side(d) + 1 - 2 * core).wait_recv()

    def slab_copies(s, own=False):
        slot = lax.rem(s, 2) if not own else 0
        return (
            pltpu.make_async_copy(
                wg_ref if own else gate_all.at[at_place(-s)], g_buf.at[slot], local_sem.at[2, slot]
            ),
            pltpu.make_async_copy(
                wu_ref if own else up_all.at[at_place(s)], u_buf.at[slot], local_sem.at[3, slot]
            ),
        )

    def multiply(s, slot, start, last):
        behind = pl.ds(pl.multiple_of(at_place(-s) * part, part), part)
        ahead = pl.ds(pl.multiple_of(at_place(s) * part, part), part)

        def one(r, carry):
            gate = jnp.dot(x_s[r, :, behind], g_buf[slot], preferred_element_type=F32)
            up = jnp.dot(x_s[r, :, ahead], u_buf[slot], preferred_element_type=F32)
            if not start:
                gate += gate_s[r]
                up += up_s[r]
            if last:
                hid_s[r] = (gate / (1.0 + jnp.exp(-gate)) * up).astype(BF16)
            else:
                gate_s[r] = gate
                up_s[r] = up
            return carry

        lax.fori_loop(0, n_tp, one, 0)

    ready = serviced // 2
    for copy in slab_copies(jnp.int32(0), True):
        copy.start()
    for copy in slab_copies(jnp.int32(0), True):
        copy.wait()
    for copy in slab_copies(jnp.int32(1)):
        copy.start()
    multiply(jnp.int32(0), 0, True, False)

    def middle(s, carry):
        for copy in slab_copies(s):
            copy.wait()

        @pl.when(s >= ready)
        def _():
            ring_event(2 * s)
            ring_event(2 * s + 1)

        for copy in slab_copies(s + 1):
            copy.start()
        multiply(s, lax.rem(s, 2), False, False)
        return carry

    lax.fori_loop(1, n_sp - 1, middle, 0)
    for copy in slab_copies(jnp.int32(n_sp - 1)):
        copy.wait()
    multiply(jnp.int32(n_sp - 1), (n_sp - 1) % 2, False, True)

    def down_load(k, own=False):
        slot = lax.rem(k, 2) if not own else 0
        hop = (k + 1) // 2
        owner = at_place(jnp.where(lax.rem(k, 2) == 1, -hop, hop))
        return pltpu.make_async_copy(
            wd_ref if own else down_all.at[owner], g_buf.at[slot], local_sem.at[2, slot]
        )

    def down_arrive(k):
        hop = (k + 1) // 2

        @pl.when(lax.rem(k, 2) == 1)
        def _():
            down_ahead(hop).wait_recv()

            @pl.when(hop < forward)
            def _():
                down_ahead(hop + 1).start()

        @pl.when(lax.rem(k, 2) == 0)
        def _():
            down_back(hop).wait_recv()

            @pl.when(hop < backward)
            def _():
                down_back(hop + 1).start()

    def pair_copy(k):
        return remote(
            pair_out.at[k], pair_in.at[k], pair_sem.at[0, k], pair_sem.at[1, k], to_partner
        )

    def cross_copy(k, d):
        return remote(
            cross_out.at[k, d - 1],
            cross_in.at[k, d - 1],
            cross_sem.at[0, k, d],
            cross_sem.at[1, k, d],
            to_side(d),
        )

    def make(k):
        slot = lax.rem(k, 2)

        def one(x, carry):
            away = lax.dot_general(
                hid_s[2 * x + 1 - core], g_buf[slot], COLS, preferred_element_type=F32
            )
            pair_out[k, x] = away.astype(BF16)
            return carry

        lax.fori_loop(0, n_x, one, 0)

        def two(x, carry):
            keep_s[slot, x] = lax.dot_general(
                hid_s[2 * x + core], g_buf[slot], COLS, preferred_element_type=F32
            )
            return carry

        lax.fori_loop(0, n_x, two, 0)
        pair_copy(k).start()

    def combine(k):
        slot = lax.rem(k, 2)
        pair_copy(k).wait_recv()
        for d in range(1, n_x):
            x = lax.rem(x_at + d, n_x)
            cross_out[k, d - 1] = (keep_s[slot, x] + pair_in[k, x].astype(F32)).astype(BF16)
            cross_copy(k, d).start()
        owner = at_place(jnp.where(lax.rem(k, 2) == 1, -((k + 1) // 2), (k + 1) // 2))
        span = pl.ds(pl.multiple_of(owner * part, part), part)
        mixed = keep_s[slot, x_at] + pair_in[k, x_at].astype(F32)
        stream_s[:, span] = stream_s[:, span] + 0.5 * mixed

    def deliver(k):
        owner = at_place(jnp.where(lax.rem(k, 2) == 1, -((k + 1) // 2), (k + 1) // 2))
        span = pl.ds(pl.multiple_of(owner * part, part), part)
        total = stream_s[:, span]
        for d in range(1, n_x):
            cross_copy(k, d).wait_recv()
            total += 0.5 * cross_in[k, d - 1].astype(F32)
        o_ref[:, span] = total.astype(BF16)

    down_load(jnp.int32(0), True).start()
    down_load(jnp.int32(0), True).wait()

    def down_step(k, carry):
        @pl.when(jnp.logical_and(k > 0, k < n_sp))
        def _():
            down_arrive(k)
            down_load(k).start()

        @pl.when(jnp.logical_and(k > 0, k <= n_sp))
        def _():
            combine(k - 1)

        @pl.when(k > 1)
        def _():
            deliver(k - 2)

        @pl.when(jnp.logical_and(k > 0, k < n_sp))
        def _():
            down_load(k).wait()

        @pl.when(k < n_sp)
        def _():
            make(k)

        return carry

    lax.fori_loop(0, n_sp + 2, down_step, 0)

    def sent_ring(e, carry):
        for copy in ring_copies(e):
            copy.wait_send()
        return carry

    lax.fori_loop(0, events, sent_ring, 0)

    def sent_hop(hop, carry):
        down_ahead(hop).wait_send()

        @pl.when(hop <= backward)
        def _():
            down_back(hop).wait_send()

        def one(way, carry):
            lat_hop(hop, way).wait_send()
            lat_pair_copy(hop, way, mine).wait_send()
            for d in range(1, n_x):
                lat_side_copy(hop, way, d, mine).wait_send()
                lat_relay_copy(hop, way, d, from_side(d)).wait_send()
            return carry

        lax.fori_loop(0, ways(hop), one, 0)
        return carry

    lax.fori_loop(1, forward + 1, sent_hop, 0)
    for kind in range(3):
        for d in range(1, n_x) if kind else range(1):
            wo_copy(kind, d, mine).wait_send()
            x_copy(kind, d, mine).wait_send()
    for d in range(1, n_tp):
        trade(d).wait_send()

    def sent_sum(k, carry):
        pair_copy(k).wait_send()
        for d in range(1, n_x):
            cross_copy(k, d).wait_send()
        return carry

    lax.fori_loop(0, n_sp, sent_sum, 0)


def layer(n_sp, n_tp, resid, qn, qr, latent, key_rope, freq, gain, mix, w_both, w_out, wg, wu, wd):
    rows = qr.shape[0]
    heads, rank, _ = w_both.shape
    share, depth = resid.shape
    part, units = wg.shape
    n_x = n_tp // 2
    forward = n_sp // 2
    tile = divisor(rows, (512, 256, 128))
    chunk = divisor(rows, (512, 256, 128))
    wide = divisor(depth, (256, 128))
    vmem = pl.BlockSpec(memory_space=pltpu.VMEM)
    anywhere = pl.BlockSpec(memory_space=pl.ANY)
    dma = pltpu.SemaphoreType.DMA
    results = pl.pallas_call(
        functools.partial(layer_kernel, n_sp, n_tp, tile, chunk),
        out_shape=(
            jax.ShapeDtypeStruct((share, depth), BF16),
            jax.ShapeDtypeStruct((n_sp, part, units), BF16),
            jax.ShapeDtypeStruct((n_sp, part, units), BF16),
            jax.ShapeDtypeStruct((n_sp, part, units), BF16),
            jax.ShapeDtypeStruct((n_tp, heads * VDIM, depth), BF16),
        ),
        in_specs=[vmem] * 9 + [anywhere] * 4,
        out_specs=(vmem, anywhere, anywhere, anywhere, anywhere),
        scratch_shapes=[
            pltpu.VMEM((n_sp, rows, rank + LANES), BF16),
            pltpu.VMEM((heads, rows, NOPE + LANES), BF16),
            pltpu.VMEM((heads, rows, NOPE + LANES), BF16),
            pltpu.VMEM((heads, VDIM + ONES, rows), BF16),
            pltpu.VMEM((heads, 8, rows), F32),
            pltpu.VMEM((heads, VDIM + ONES, rows), F32),
            pltpu.VMEM((2, rows, tile), F32),
            pltpu.VMEM((2, 8, tile), F32),
            pltpu.VMEM((n_tp, share, heads * VDIM), BF16),
            pltpu.VMEM((n_tp, share, heads * VDIM), BF16),
            pltpu.VMEM((2, n_tp, heads * VDIM, wide), BF16),
            pltpu.VMEM((n_tp, share, depth), BF16),
            pltpu.VMEM((share, depth), F32),
            pltpu.VMEM((n_tp, share, units), F32),
            pltpu.VMEM((n_tp, share, units), F32),
            pltpu.VMEM((n_tp, share, units), BF16),
            pltpu.VMEM((2, part, units), BF16),
            pltpu.VMEM((2, part, units), BF16),
            pltpu.VMEM((2, n_x, share, part), F32),
            pltpu.VMEM((n_sp, n_x, share, part), BF16),
            pltpu.VMEM((n_sp, n_x, share, part), BF16),
            pltpu.VMEM((n_sp, n_x - 1, share, part), BF16),
            pltpu.VMEM((n_sp, n_x - 1, share, part), BF16),
            dma((2, 2, forward + 1)),
            dma((2, 2, forward + 1)),
            dma((2, 2, forward + 1, n_x)),
            dma((2, 2, forward + 1, n_x)),
            dma((2, 3, n_x)),
            dma((4, 2 * (n_sp - 1))),
            dma((4, forward + 1)),
            dma((2, n_tp)),
            dma((2, 3, n_x)),
            dma((2, n_sp)),
            dma((2, n_sp, n_x)),
            dma((4, 2)),
        ],
        compiler_params=pltpu.CompilerParams(
            collective_id=0, has_side_effects=True, vmem_limit_bytes=67043328
        ),
    )(resid, qn, qr, latent, key_rope, freq, gain, mix, w_both, w_out, wg, wu, wd)
    return results[0]


def on_device(
    n_sp,
    n_tp,
    resid,
    query_nope,
    query_rope,
    latent,
    key_rope,
    latent_gain,
    w_key,
    w_value,
    w_out,
    mix_gain,
    w_gate,
    w_up,
    w_down,
):
    head_count = query_nope.shape[1] // NOPE
    rank = latent.shape[1]
    half_width = ROPE // 2
    frequency = theta_base ** (-2.0 * jnp.arange(half_width).astype(F32) / ROPE)
    frequency = jnp.tile(frequency, LANES // half_width)[None, :]
    w_both = jnp.concatenate(
        [w_key.reshape(rank, head_count, NOPE), w_value.reshape(rank, head_count, VDIM)], axis=-1
    ).transpose(1, 0, 2)
    return layer(
        n_sp,
        n_tp,
        resid,
        query_nope,
        query_rope,
        latent,
        key_rope,
        frequency,
        latent_gain[None, :],
        mix_gain[None, :],
        w_both,
        w_out,
        w_gate,
        w_up,
        w_down,
    )


def solution(mesh):
    return jax.shard_map(
        functools.partial(on_device, mesh.shape["sp"], mesh.shape["tp"]),
        mesh=mesh,
        in_specs=(
            P(("sp", "tp"), None),
            P("sp", "tp"),
            P("sp", "tp"),
            P("sp", None),
            P("sp", None),
            P(),
            P(None, "tp"),
            P(None, "tp"),
            P("tp", None),
            P(),
            P("sp", "tp"),
            P("sp", "tp"),
            P("sp", "tp"),
        ),
        out_specs=P(("sp", "tp"), None),
        check_vma=False,
    )
```

```python
import functools

import jax
import jax.numpy as jnp
import numpy as np
from jax import lax
from jax.experimental import pallas as pl
from jax.experimental.pallas import tpu as pltpu
from jax.sharding import PartitionSpec as P

NOPE = 128
ROPE = 64
VDIM = 128
LANES = 128
ONES = 16

norm_eps = 1e-06
masked_score = -1e30
theta_base = 10000.0
LOG2E = 1.4426950408889634
COLS = (((1,), (1,)), ((), ()))
MIB = 1024 * 1024
MESH = pl.DeviceIdType.MESH
F32 = jnp.float32
BF16 = jnp.bfloat16


def ring_order(count):
    narrow = 1
    while (2 * narrow) ** 2 <= count and count % (2 * narrow) == 0:
        narrow *= 2
    long = count // narrow
    if narrow == 1 or long % 2:
        return list(range(count))
    order = []
    for row in range(long):
        columns = range(1, narrow) if row % 2 == 0 else range(narrow - 1, 0, -1)
        order += [row * narrow + column for column in columns]
    return order + [row * narrow for row in reversed(range(long))]


def divisor(size, choices):
    return next(choice for choice in choices if size % choice == 0)


def pick(table, index):
    found = jnp.int32(0)
    for i, value in enumerate(table):
        found = jnp.where(index == i, jnp.int32(value), found)
    return found


def remote(src, dst, send, recv, where):
    return pltpu.make_async_remote_copy(
        src_ref=src, dst_ref=dst, send_sem=send, recv_sem=recv, device_id=where, device_id_type=MESH
    )


def layer_kernel(
    n_sp,
    n_tp,
    tile,
    chunk,
    resid_ref,
    qn_ref,
    qr_ref,
    lat_ref,
    kr_ref,
    freq_ref,
    gain_ref,
    mix_ref,
    wk_ref,
    wv_ref,
    wo_ref,
    wg_ref,
    wu_ref,
    wd_ref,
    o_ref,
    gate_all,
    up_all,
    down_all,
    wo_all,
    lat_all,
    wb_s,
    q_s,
    k_s,
    v_s,
    m_s,
    acc_s,
    s_s,
    mx_s,
    ho_s,
    tr_s,
    wo_s,
    x_s,
    stream_s,
    gate_s,
    up_s,
    hid_s,
    g_buf,
    u_buf,
    keep_s,
    pair_out,
    pair_in,
    cross_out,
    cross_in,
    lat_ring,
    lat_pair,
    lat_side,
    lat_relay,
    wo_sem,
    ring_sem,
    down_sem,
    trade_sem,
    x_sem,
    pair_sem,
    cross_sem,
    local_sem,
    wo_local,
):
    me = lax.axis_index("sp")
    mine = lax.axis_index("tp")
    rows = qr_ref.shape[0]
    heads = wb_s.shape[0]
    rank = wb_s.shape[1]
    depth = resid_ref.shape[1]
    share = rows // n_tp
    part = wg_ref.shape[0]
    half = part // 2
    n_x = n_tp // 2
    x_at, core = mine // 2, lax.rem(mine, 2)
    partner = mine + 1 - 2 * core
    forward = n_sp // 2
    backward = n_sp - 1 - forward
    events = 2 * (n_sp - 1)

    order = ring_order(n_sp)
    place = pick([order.index(i) for i in range(n_sp)], me)

    def at_place(offset):
        return pick(order, lax.rem(place + offset + 2 * n_sp, n_sp))

    right, left = at_place(1), at_place(-1)
    to_right, to_left = {"sp": right, "tp": mine}, {"sp": left, "tp": mine}
    to_partner = {"sp": me, "tp": partner}

    def side(d):
        return lax.rem(x_at + d, n_x) * 2 + core

    def to_side(d):
        return {"sp": me, "tp": side(d)}

    def from_side(d):
        return lax.rem(x_at - d + n_x, n_x) * 2 + core

    barrier = pltpu.get_barrier_semaphore()
    pl.semaphore_signal(barrier, inc=1, device_id=to_right, device_id_type=MESH)
    pl.semaphore_signal(barrier, inc=1, device_id=to_left, device_id_type=MESH)
    for d in range(1, n_tp):
        peer = {"sp": me, "tp": lax.rem(mine + d, n_tp)}
        pl.semaphore_signal(barrier, inc=1, device_id=peer, device_id_type=MESH)
    pl.semaphore_wait(barrier, n_tp + 1)

    def piece(ref, i):
        return ref.at[pl.ds(pl.multiple_of(i * half, half), half), :]

    def ring_copies(e, first=False):
        hop, i = e // 2 + 1, lax.rem(e, 2)
        behind, beyond = at_place(1 - hop), at_place(hop - 1)
        return (
            remote(
                piece(wg_ref if first else gate_all.at[behind], i),
                piece(gate_all.at[behind], i),
                ring_sem.at[0, e],
                ring_sem.at[1, e],
                to_right,
            ),
            remote(
                piece(wu_ref if first else up_all.at[beyond], i),
                piece(up_all.at[beyond], i),
                ring_sem.at[2, e],
                ring_sem.at[3, e],
                to_left,
            ),
        )

    def down_copies(f, first=False):
        hop, i = f // 2 + 1, lax.rem(f, 2)
        behind, beyond = at_place(1 - hop), at_place(hop - 1)
        return (
            remote(
                piece(wd_ref if first else down_all.at[behind], i),
                piece(down_all.at[behind], i),
                down_sem.at[0, f],
                down_sem.at[1, f],
                to_right,
            ),
            remote(
                piece(wd_ref if first else down_all.at[beyond], i),
                piece(down_all.at[beyond], i),
                down_sem.at[2, f],
                down_sem.at[3, f],
                to_left,
            ),
        )

    def down_valid(f):
        last = f // 2 + 1 == forward
        inside = f // 2 + 1 <= forward
        even = lax.rem(f, 2) == 0
        ahead = jnp.logical_and(inside, jnp.logical_or(jnp.logical_not(last), even))
        back = jnp.logical_and(
            inside, jnp.logical_or(jnp.logical_not(last), jnp.logical_not(even))
        )
        return ahead, back

    def down_event(f):
        for copy, valid in zip(down_copies(f), down_valid(f)):

            @pl.when(valid)
            def _():
                copy.wait_recv()

        for way, valid in enumerate(down_valid(f + 2)):

            @pl.when(valid)
            def _():
                down_copies(f + 2)[way].start()

    def ring_event(e):
        for copy in ring_copies(e):
            copy.wait_recv()

        @pl.when(e + 2 < events)
        def _():
            for copy in ring_copies(e + 2):
                copy.start()

        @pl.when(e == events - 3)
        def _():
            for f in range(2):
                for copy in down_copies(jnp.int32(f), True):
                    copy.start()

    def quarter(owner, t):
        return lat_all.at[owner, pl.ds(pl.multiple_of(t * share, share), share), :]

    def lat_hop(hop, way):
        owner = at_place(jnp.where(way == 0, 1 - hop, hop - 1))
        where = {"sp": jnp.where(way == 0, right, left), "tp": mine}
        return remote(
            quarter(owner, mine),
            quarter(owner, mine),
            lat_ring.at[0, way, hop],
            lat_ring.at[1, way, hop],
            where,
        )

    def lat_owner(hop, way):
        return at_place(jnp.where(way == 0, -hop, hop))

    def lat_pair_copy(hop, way, t):
        owner = lat_owner(hop, way)
        return remote(
            quarter(owner, t),
            quarter(owner, t),
            lat_pair.at[0, way, hop],
            lat_pair.at[1, way, hop],
            to_partner,
        )

    def lat_side_copy(hop, way, d, t):
        owner = lat_owner(hop, way)
        return remote(
            quarter(owner, t),
            quarter(owner, t),
            lat_side.at[0, way, hop, d],
            lat_side.at[1, way, hop, d],
            to_side(d),
        )

    def lat_relay_copy(hop, way, d, t):
        owner = lat_owner(hop, way)
        return remote(
            quarter(owner, t),
            quarter(owner, t),
            lat_relay.at[0, way, hop, d],
            lat_relay.at[1, way, hop, d],
            to_partner,
        )

    def ways(hop):
        return jnp.where(hop <= backward, 2, 1)

    def lat_forward(hop):
        def one(way, carry):
            lat_hop(hop, way).wait_recv()

            @pl.when(hop + 1 <= jnp.where(way == 0, forward, backward))
            def _():
                lat_hop(hop + 1, way).start()

            for d in range(1, n_x):
                lat_side_copy(hop, way, d, mine).start()
            lat_pair_copy(hop, way, mine).start()
            return carry

        lax.fori_loop(0, ways(hop), one, 0)

    def lat_pass(hop):
        def one(way, carry):
            for d in range(1, n_x):
                lat_side_copy(hop, way, d, from_side(d)).wait_recv()
                lat_relay_copy(hop, way, d, from_side(d)).start()
            return carry

        lax.fori_loop(0, ways(hop), one, 0)

    def lat_ready(hop, way):
        lat_pair_copy(hop, way, partner).wait_recv()
        for d in range(1, n_x):
            lat_relay_copy(hop, way, d, from_side(d) + 1 - 2 * core).wait_recv()

    def wo_copy(kind, d, t, src=None):
        where = to_partner if kind != 1 else to_side(d)
        return remote(
            wo_all.at[t] if src is None else src,
            wo_all.at[t],
            wo_sem.at[0, kind, d],
            wo_sem.at[1, kind, d],
            where,
        )

    def rotated(values, span):
        first = first_row + span
        position = (first + lax.broadcasted_iota(jnp.int32, values.shape, 0)).astype(F32)
        angle = position * freq_ref[...]
        front = lax.rem(lax.broadcasted_iota(jnp.int32, values.shape, 1), ROPE) < ROPE // 2
        return angle, front

    def turn(values, cosine, sine, front):
        other = jnp.where(
            front,
            pltpu.roll(values, LANES - ROPE // 2, 1),
            pltpu.roll(values, ROPE // 2, 1),
        )
        return values * cosine + other * sine

    first_row = me * rows

    def prepare(i, carry):
        start = pl.multiple_of(i * share, share)
        span = pl.ds(start, share)
        key = kr_ref[span, :].astype(F32)
        key = jnp.concatenate([key, key], axis=1)
        angle, front = rotated(key, start)
        cosine = jnp.cos(angle)
        sine = jnp.sin(angle)
        sine = jnp.where(front, -sine, sine)
        lat_all[me, span, rank:] = turn(key, cosine, sine, front).astype(BF16)
        latent = lat_ref[span, :].astype(F32)
        power = jnp.mean(latent * latent, axis=1, keepdims=True)
        latent = latent * lax.rsqrt(power + norm_eps) * gain_ref[...]
        lat_all[me, span, :rank] = latent.astype(BF16)
        for j in range(heads // 2):
            pair = qr_ref[span, j * LANES : (j + 1) * LANES].astype(F32)
            pair = turn(pair, cosine, sine, front)
            q_s[2 * j, span, NOPE:] = pair.astype(BF16)
            q_s[2 * j + 1, span, NOPE:] = pltpu.roll(pair, ROPE, 1).astype(BF16)
        for h in range(heads):
            q_s[h, span, :NOPE] = qn_ref[span, h * NOPE : (h + 1) * NOPE]
        return carry

    for copy in ring_copies(jnp.int32(0), True):
        copy.start()
    for h in range(heads):
        wb_s[h, :, :NOPE] = wk_ref[:, h * NOPE : (h + 1) * NOPE]
        wb_s[h, :, NOPE:] = wv_ref[:, h * VDIM : (h + 1) * VDIM]
    lax.fori_loop(0, n_tp, prepare, 0)
    lat_hop(1, jnp.int32(0)).start()
    if backward:
        lat_hop(1, jnp.int32(1)).start()
    for copy in ring_copies(jnp.int32(1), True):
        copy.start()

    tiles = rows // tile
    chunks = rows // chunk
    total = heads * tiles
    scale = (NOPE + ROPE) ** (-0.5) * LOG2E

    m_s[...] = jnp.full_like(m_s, masked_score)
    acc_s[...] = jnp.zeros_like(acc_s)
    for h in range(heads):
        v_s[h, VDIM:, :] = jnp.ones((ONES, rows), BF16)

    def project(owner):
        def one(h, carry):
            both = jnp.dot(
                lat_all[owner, :, :rank], wb_s[h], preferred_element_type=F32
            ).astype(BF16)
            k_s[h, :, :NOPE] = both[:, :NOPE]
            k_s[h, :, NOPE:] = lat_all[owner, :, rank:]
            v_s[h, :VDIM, :] = both[:, NOPE:].T
            return carry

        lax.fori_loop(0, heads, one, 0)

    def span_of(t):
        return pl.ds(t * tile if isinstance(t, int) else pl.multiple_of(t * tile, tile), tile)

    def score(h, t, c, slot, top, diagonal):
        keys = slice(c * chunk, (c + 1) * chunk)
        scores = scale * lax.dot_general(
            k_s[h, keys, : NOPE + ROPE],
            q_s[h, span_of(t), : NOPE + ROPE],
            COLS,
            preferred_element_type=F32,
        )
        if diagonal:
            row = t * tile + lax.broadcasted_iota(jnp.int32, scores.shape, 1)
            col = c * chunk + lax.broadcasted_iota(jnp.int32, scores.shape, 0)
            scores = jnp.where(col <= row, scores, masked_score)
        s_s[slot, keys, :] = scores
        peak = jnp.max(scores.reshape(chunk // 8, 8, tile), axis=0)
        return peak if top is None else jnp.maximum(top, peak)

    def advance(h, t, peak):
        old = m_s[h, :, span_of(t)]
        top = jnp.maximum(old, jnp.max(peak, axis=0, keepdims=True))
        m_s[h, :, span_of(t)] = top
        return top[:1], jnp.exp2(old - top)[:1]

    def fold(h, c, slot, top, mixed):
        keys = slice(c * chunk, (c + 1) * chunk)
        weights = jnp.exp2(s_s[slot, keys, :] - top).astype(BF16)
        term = jnp.dot(v_s[h, :, keys], weights, preferred_element_type=F32)
        return term if mixed is None else mixed + term

    def finish(h, t, factor, mixed):
        acc_s[h, :, span_of(t)] = acc_s[h, :, span_of(t)] * factor + mixed

    project(me)

    def own_head(h, carry):
        for t in range(tiles):
            peak = mixed = None
            limit = -(-(t + 1) * tile // chunk)
            for c in range(limit):
                peak = score(h, t, c, t % 2, peak, (c + 1) * chunk > t * tile)
            top, factor = advance(h, t, peak)
            for c in range(limit):
                mixed = fold(h, c, t % 2, top, mixed)
            finish(h, t, factor, mixed)
        return carry

    lax.fori_loop(0, heads, own_head, 0)

    def attend(owner):
        project(owner)
        peak = None
        for c in range(chunks):
            peak = score(0, 0, c, 0, peak, False)
        mx_s[0] = peak

        def one(i, slot):
            h, t = i // tiles, lax.rem(i, tiles)
            later = jnp.minimum(i + 1, total - 1)
            next_h, next_t = later // tiles, lax.rem(later, tiles)
            top, factor = advance(h, t, mx_s[slot])
            peak = mixed = None
            for c in range(chunks):
                peak = score(next_h, next_t, c, 1 - slot, peak, False)
                mixed = fold(h, c, slot, top, mixed)
            mx_s[1 - slot] = peak
            finish(h, t, factor, mixed)

        def two(i, carry):
            one(2 * i, 0)
            one(2 * i + 1, 1)
            return carry

        lax.fori_loop(0, total // 2, two, 0)

    lat_forward(jnp.int32(1))
    lat_pass(jnp.int32(1))

    def block(i, carry):
        hop = i // 2 + 1
        way = lax.rem(i, 2)

        @pl.when(way < ways(hop))
        def _():
            lat_ready(hop, way)
            owner = lat_owner(hop, way)

            @pl.when(owner < me)
            def _():
                attend(owner)

        @pl.when(jnp.logical_and(way == 0, hop < forward))
        def _():
            lat_forward(hop + 1)

        @pl.when(i == 2 * forward - 4)
        def _():
            for d in range(1, n_x):
                wo_copy(1, d, mine, wo_ref).start()
            wo_copy(0, 0, mine, wo_ref).start()

        @pl.when(jnp.logical_and(way == 1, hop < forward))
        def _():
            lat_pass(hop + 1)

        ring_event(i)
        return carry

    lax.fori_loop(0, 2 * forward, block, 0)
    serviced = 2 * forward

    def finish_head(h):
        done = acc_s[h]
        out = (done[:VDIM] / done[VDIM : VDIM + 1]).T.astype(BF16)
        for r in range(n_tp):
            ho_s[r, :, h * VDIM : (h + 1) * VDIM] = out[r * share : (r + 1) * share]

    for h in range(heads):
        finish_head(h)
    tr_s[mine] = ho_s[mine]

    def trade(d):
        target = lax.rem(mine + d, n_tp)
        return remote(
            ho_s.at[target],
            tr_s.at[mine],
            trade_sem.at[0, d],
            trade_sem.at[1, d],
            {"sp": me, "tp": target},
        )

    def traded(d):
        source = lax.rem(mine - d + n_tp, n_tp)
        return remote(
            ho_s.at[source],
            tr_s.at[source],
            trade_sem.at[0, d],
            trade_sem.at[1, d],
            {"sp": me, "tp": source},
        )

    for d in range(1, n_tp):
        trade(d).start()
    for d in range(1, n_x):
        wo_copy(1, d, from_side(d)).wait_recv()
        wo_copy(2, d, from_side(d)).start()
    wo_copy(0, 0, partner).wait_recv()
    for d in range(1, n_x):
        wo_copy(2, d, from_side(d) + 1 - 2 * core).wait_recv()

    wide = wo_s.shape[3]
    columns = depth // wide

    def wo_loads(j):
        span = pl.ds(j * wide, wide)
        own = pltpu.make_async_copy(
            wo_ref.at[:, span], wo_s.at[j % 2, 0], wo_local.at[0, j % 2]
        )
        others = [
            pltpu.make_async_copy(
                wo_all.at[lax.rem(mine + d, n_tp), :, span],
                wo_s.at[j % 2, d],
                wo_local.at[d, j % 2],
            )
            for d in range(1, n_tp)
        ]
        return [own] + others

    for copy in wo_loads(0):
        copy.start()
    for d in range(1, n_tp):
        traded(d).wait_recv()
    for j in range(columns):
        for copy in wo_loads(j):
            copy.wait()
        if j + 1 < columns:
            for copy in wo_loads(j + 1):
                copy.start()
        proj = resid_ref[:, j * wide : (j + 1) * wide].astype(F32)
        for d in range(n_tp):
            group = lax.rem(mine + d, n_tp)
            proj += jnp.dot(tr_s[group], wo_s[j % 2, d], preferred_element_type=F32)
        stream_s[:, j * wide : (j + 1) * wide] = proj

    strip = divisor(share, (64, 32, 16, 8))

    def normalise(i, carry):
        span = pl.ds(pl.multiple_of(i * strip, strip), strip)
        stream = stream_s[span, :]
        power = jnp.mean(stream * stream, axis=1, keepdims=True)
        x_s[mine, span, :] = (stream * lax.rsqrt(power + norm_eps) * mix_ref[...]).astype(BF16)
        return carry

    lax.fori_loop(0, share // strip, normalise, 0)

    def x_copy(kind, d, t):
        where = to_partner if kind != 1 else to_side(d)
        return remote(x_s.at[t], x_s.at[t], x_sem.at[0, kind, d], x_sem.at[1, kind, d], where)

    for d in range(1, n_x):
        x_copy(1, d, mine).start()
    x_copy(0, 0, mine).start()
    for _ in range(2):
        ring_event(jnp.int32(serviced))
        serviced += 1
    for d in range(1, n_x):
        x_copy(1, d, from_side(d)).wait_recv()
        x_copy(2, d, from_side(d)).start()
    for _ in range(2):
        ring_event(jnp.int32(serviced))
        serviced += 1
    x_copy(0, 0, partner).wait_recv()
    for d in range(1, n_x):
        x_copy(2, d, from_side(d) + 1 - 2 * core).wait_recv()

    def slab_copies(s, own=False):
        slot = lax.rem(s, 2) if not own else 0
        return (
            pltpu.make_async_copy(
                wg_ref if own else gate_all.at[at_place(-s)], g_buf.at[slot], local_sem.at[2, slot]
            ),
            pltpu.make_async_copy(
                wu_ref if own else up_all.at[at_place(s)], u_buf.at[slot], local_sem.at[3, slot]
            ),
        )

    def multiply(s, slot, start, last):
        behind = pl.ds(pl.multiple_of(at_place(-s) * part, part), part)
        ahead = pl.ds(pl.multiple_of(at_place(s) * part, part), part)

        def one(r, carry):
            gate = jnp.dot(x_s[r, :, behind], g_buf[slot], preferred_element_type=F32)
            up = jnp.dot(x_s[r, :, ahead], u_buf[slot], preferred_element_type=F32)
            if not start:
                gate += gate_s[r]
                up += up_s[r]
            if last:
                hid_s[r] = (gate / (1.0 + jnp.exp(-gate)) * up).astype(BF16)
            else:
                gate_s[r] = gate
                up_s[r] = up
            return carry

        lax.fori_loop(0, n_tp, one, 0)

    ready = serviced // 2
    for copy in slab_copies(jnp.int32(0), True):
        copy.start()
    for copy in slab_copies(jnp.int32(0), True):
        copy.wait()
    for copy in slab_copies(jnp.int32(1)):
        copy.start()
    multiply(jnp.int32(0), 0, True, False)

    def middle(s, carry):
        for copy in slab_copies(s):
            copy.wait()

        @pl.when(s >= ready)
        def _():
            ring_event(2 * s)
            ring_event(2 * s + 1)

        for copy in slab_copies(s + 1):
            copy.start()
        multiply(s, lax.rem(s, 2), False, False)
        return carry

    lax.fori_loop(1, n_sp - 1, middle, 0)
    for copy in slab_copies(jnp.int32(n_sp - 1)):
        copy.wait()
    multiply(jnp.int32(n_sp - 1), (n_sp - 1) % 2, False, True)

    def down_load(k, own=False):
        slot = lax.rem(k, 2) if not own else 0
        hop = (k + 1) // 2
        owner = at_place(jnp.where(lax.rem(k, 2) == 1, -hop, hop))
        return pltpu.make_async_copy(
            wd_ref if own else down_all.at[owner], g_buf.at[slot], local_sem.at[2, slot]
        )

    def down_arrive(k):
        down_event(k - 1)
        down_event(k)

    def pair_copy(k):
        return remote(
            pair_out.at[k], pair_in.at[k], pair_sem.at[0, k], pair_sem.at[1, k], to_partner
        )

    def cross_copy(k, d):
        return remote(
            cross_out.at[k, d - 1],
            cross_in.at[k, d - 1],
            cross_sem.at[0, k, d],
            cross_sem.at[1, k, d],
            to_side(d),
        )

    def make(k):
        slot = lax.rem(k, 2)

        def one(x, carry):
            away = lax.dot_general(
                hid_s[2 * x + 1 - core], g_buf[slot], COLS, preferred_element_type=F32
            )
            pair_out[k, x] = away.astype(BF16)
            return carry

        lax.fori_loop(0, n_x, one, 0)

        def two(x, carry):
            keep_s[slot, x] = lax.dot_general(
                hid_s[2 * x + core], g_buf[slot], COLS, preferred_element_type=F32
            )
            return carry

        lax.fori_loop(0, n_x, two, 0)
        pair_copy(k).start()

    def combine(k):
        slot = lax.rem(k, 2)
        pair_copy(k).wait_recv()
        for d in range(1, n_x):
            x = lax.rem(x_at + d, n_x)
            cross_out[k, d - 1] = (keep_s[slot, x] + pair_in[k, x].astype(F32)).astype(BF16)
            cross_copy(k, d).start()
        owner = at_place(jnp.where(lax.rem(k, 2) == 1, -((k + 1) // 2), (k + 1) // 2))
        span = pl.ds(pl.multiple_of(owner * part, part), part)
        mixed = keep_s[slot, x_at] + pair_in[k, x_at].astype(F32)
        stream_s[:, span] = stream_s[:, span] + 0.5 * mixed

    def deliver(k):
        owner = at_place(jnp.where(lax.rem(k, 2) == 1, -((k + 1) // 2), (k + 1) // 2))
        span = pl.ds(pl.multiple_of(owner * part, part), part)
        total = stream_s[:, span]
        for d in range(1, n_x):
            cross_copy(k, d).wait_recv()
            total += 0.5 * cross_in[k, d - 1].astype(F32)
        o_ref[:, span] = total.astype(BF16)

    down_load(jnp.int32(0), True).start()
    down_load(jnp.int32(0), True).wait()

    def down_step(k, carry):
        @pl.when(jnp.logical_and(lax.rem(k, 2) == 1, k < n_sp))
        def _():
            down_arrive(k)
            down_load(k).start()

            @pl.when(k + 1 < n_sp)
            def _():
                down_load(k + 1).start()

        @pl.when(jnp.logical_and(k > 0, k < n_sp))
        def _():
            down_load(k).wait()

        @pl.when(k < n_sp)
        def _():
            make(k)

        @pl.when(jnp.logical_and(k > 0, k <= n_sp))
        def _():
            combine(k - 1)

        @pl.when(k > 1)
        def _():
            deliver(k - 2)

        return carry

    lax.fori_loop(0, n_sp + 2, down_step, 0)

    def sent_ring(e, carry):
        for copy in ring_copies(e):
            copy.wait_send()
        return carry

    lax.fori_loop(0, events, sent_ring, 0)

    def sent_hop(hop, carry):
        for i in range(2):
            f = 2 * (hop - 1) + i
            for copy, valid in zip(down_copies(f), down_valid(f)):

                @pl.when(valid)
                def _():
                    copy.wait_send()

        def one(way, carry):
            lat_hop(hop, way).wait_send()
            lat_pair_copy(hop, way, mine).wait_send()
            for d in range(1, n_x):
                lat_side_copy(hop, way, d, mine).wait_send()
                lat_relay_copy(hop, way, d, from_side(d)).wait_send()
            return carry

        lax.fori_loop(0, ways(hop), one, 0)
        return carry

    lax.fori_loop(1, forward + 1, sent_hop, 0)
    for kind in range(3):
        for d in range(1, n_x) if kind else range(1):
            wo_copy(kind, d, mine).wait_send()
            x_copy(kind, d, mine).wait_send()
    for d in range(1, n_tp):
        trade(d).wait_send()

    def sent_sum(k, carry):
        pair_copy(k).wait_send()
        for d in range(1, n_x):
            cross_copy(k, d).wait_send()
        return carry

    lax.fori_loop(0, n_sp, sent_sum, 0)


def layer(n_sp, n_tp, resid, qn, qr, latent, key_rope, freq, gain, mix, wk, wv, w_out, wg, wu, wd):
    rows = qr.shape[0]
    heads, rank = wk.shape[1] // NOPE, wk.shape[0]
    share, depth = resid.shape
    part, units = wg.shape
    n_x = n_tp // 2
    forward = n_sp // 2
    tile = divisor(rows, (512, 256, 128))
    chunk = divisor(rows, (512, 256, 128))
    wide = divisor(depth, (256, 128))
    vmem = pl.BlockSpec(memory_space=pltpu.VMEM)
    anywhere = pl.BlockSpec(memory_space=pl.ANY)
    dma = pltpu.SemaphoreType.DMA
    results = pl.pallas_call(
        functools.partial(layer_kernel, n_sp, n_tp, tile, chunk),
        out_shape=(
            jax.ShapeDtypeStruct((share, depth), BF16),
            jax.ShapeDtypeStruct((n_sp, part, units), BF16),
            jax.ShapeDtypeStruct((n_sp, part, units), BF16),
            jax.ShapeDtypeStruct((n_sp, part, units), BF16),
            jax.ShapeDtypeStruct((n_tp, heads * VDIM, depth), BF16),
        ),
        in_specs=[vmem] * 10 + [anywhere] * 4,
        out_specs=(vmem, anywhere, anywhere, anywhere, anywhere),
        scratch_shapes=[
            pltpu.VMEM((n_sp, rows, rank + LANES), BF16),
            pltpu.VMEM((heads, rank, NOPE + VDIM), BF16),
            pltpu.VMEM((heads, rows, NOPE + LANES), BF16),
            pltpu.VMEM((heads, rows, NOPE + LANES), BF16),
            pltpu.VMEM((heads, VDIM + ONES, rows), BF16),
            pltpu.VMEM((heads, 8, rows), F32),
            pltpu.VMEM((heads, VDIM + ONES, rows), F32),
            pltpu.VMEM((2, rows, tile), F32),
            pltpu.VMEM((2, 8, tile), F32),
            pltpu.VMEM((n_tp, share, heads * VDIM), BF16),
            pltpu.VMEM((n_tp, share, heads * VDIM), BF16),
            pltpu.VMEM((2, n_tp, heads * VDIM, wide), BF16),
            pltpu.VMEM((n_tp, share, depth), BF16),
            pltpu.VMEM((share, depth), F32),
            pltpu.VMEM((n_tp, share, units), F32),
            pltpu.VMEM((n_tp, share, units), F32),
            pltpu.VMEM((n_tp, share, units), BF16),
            pltpu.VMEM((2, part, units), BF16),
            pltpu.VMEM((2, part, units), BF16),
            pltpu.VMEM((2, n_x, share, part), F32),
            pltpu.VMEM((n_sp, n_x, share, part), BF16),
            pltpu.VMEM((n_sp, n_x, share, part), BF16),
            pltpu.VMEM((n_sp, n_x - 1, share, part), BF16),
            pltpu.VMEM((n_sp, n_x - 1, share, part), BF16),
            dma((2, 2, forward + 1)),
            dma((2, 2, forward + 1)),
            dma((2, 2, forward + 1, n_x)),
            dma((2, 2, forward + 1, n_x)),
            dma((2, 3, n_x)),
            dma((4, 2 * (n_sp - 1))),
            dma((4, 2 * forward)),
            dma((2, n_tp)),
            dma((2, 3, n_x)),
            dma((2, n_sp)),
            dma((2, n_sp, n_x)),
            dma((4, 2)),
            dma((n_tp, 2)),
        ],
        compiler_params=pltpu.CompilerParams(
            collective_id=0, has_side_effects=True, vmem_limit_bytes=67043328
        ),
    )(resid, qn, qr, latent, key_rope, freq, gain, mix, wk, wv, w_out, wg, wu, wd)
    return results[0]


def on_device(
    n_sp,
    n_tp,
    resid,
    query_nope,
    query_rope,
    latent,
    key_rope,
    latent_gain,
    w_key,
    w_value,
    w_out,
    mix_gain,
    w_gate,
    w_up,
    w_down,
):
    half_width = ROPE // 2
    frequency = theta_base ** (-2.0 * np.arange(half_width) / ROPE)
    frequency = jnp.asarray(np.tile(frequency, LANES // half_width)[None, :], F32)
    return layer(
        n_sp,
        n_tp,
        resid,
        query_nope,
        query_rope,
        latent,
        key_rope,
        frequency,
        latent_gain[None, :],
        mix_gain[None, :],
        w_key,
        w_value,
        w_out,
        w_gate,
        w_up,
        w_down,
    )


def solution(mesh):
    return jax.shard_map(
        functools.partial(on_device, mesh.shape["sp"], mesh.shape["tp"]),
        mesh=mesh,
        in_specs=(
            P(("sp", "tp"), None),
            P("sp", "tp"),
            P("sp", "tp"),
            P("sp", None),
            P("sp", None),
            P(),
            P(None, "tp"),
            P(None, "tp"),
            P("tp", None),
            P(),
            P("sp", "tp"),
            P("sp", "tp"),
            P("sp", "tp"),
        ),
        out_specs=P(("sp", "tp"), None),
        check_vma=False,
    )
```

```python
import functools

import jax
import jax.numpy as jnp
import numpy as np
from jax import lax
from jax.experimental import pallas as pl
from jax.experimental.pallas import tpu as pltpu
from jax.sharding import PartitionSpec as P

NOPE = 128
ROPE = 64
VDIM = 128
LANES = 128
ONES = 16

norm_eps = 1e-06
masked_score = -1e30
theta_base = 10000.0
LOG2E = 1.4426950408889634
COLS = (((1,), (1,)), ((), ()))
MIB = 1024 * 1024
MESH = pl.DeviceIdType.MESH
F32 = jnp.float32
BF16 = jnp.bfloat16


def ring_order(count):
    narrow = 1
    while (2 * narrow) ** 2 <= count and count % (2 * narrow) == 0:
        narrow *= 2
    long = count // narrow
    if narrow == 1 or long % 2:
        return list(range(count))
    order = []
    for row in range(long):
        columns = range(1, narrow) if row % 2 == 0 else range(narrow - 1, 0, -1)
        order += [row * narrow + column for column in columns]
    return order + [row * narrow for row in reversed(range(long))]


def divisor(size, choices):
    return next(choice for choice in choices if size % choice == 0)


def pick(table, index):
    found = jnp.int32(0)
    for i, value in enumerate(table):
        found = jnp.where(index == i, jnp.int32(value), found)
    return found


def remote(src, dst, send, recv, where):
    return pltpu.make_async_remote_copy(
        src_ref=src, dst_ref=dst, send_sem=send, recv_sem=recv, device_id=where, device_id_type=MESH
    )


def layer_kernel(
    n_sp,
    n_tp,
    tile,
    chunk,
    resid_ref,
    qn_ref,
    qr_ref,
    lat_ref,
    kr_ref,
    freq_ref,
    gain_ref,
    mix_ref,
    wk_ref,
    wv_ref,
    wo_ref,
    wg_ref,
    wu_ref,
    wd_ref,
    o_ref,
    gate_all,
    up_all,
    down_all,
    wo_all,
    lat_all,
    wb_s,
    q_s,
    k_s,
    v_s,
    m_s,
    acc_s,
    s_s,
    mx_s,
    ho_s,
    tr_s,
    wo_s,
    x_s,
    stream_s,
    gate_s,
    up_s,
    hid_s,
    g_buf,
    u_buf,
    keep_s,
    pair_out,
    pair_in,
    cross_out,
    cross_in,
    lat_ring,
    lat_pair,
    lat_side,
    lat_relay,
    wo_sem,
    ring_sem,
    down_sem,
    trade_sem,
    x_sem,
    pair_sem,
    cross_sem,
    local_sem,
    wo_local,
):
    me = lax.axis_index("sp")
    mine = lax.axis_index("tp")
    rows = qr_ref.shape[0]
    heads = wb_s.shape[0]
    rank = wb_s.shape[1]
    depth = resid_ref.shape[1]
    share = rows // n_tp
    part = wg_ref.shape[0]
    half = part // 2
    n_x = n_tp // 2
    x_at, core = mine // 2, lax.rem(mine, 2)
    partner = mine + 1 - 2 * core
    forward = n_sp // 2
    backward = n_sp - 1 - forward
    events = 2 * (n_sp - 1)

    order = ring_order(n_sp)
    place = pick([order.index(i) for i in range(n_sp)], me)

    def at_place(offset):
        return pick(order, lax.rem(place + offset + 2 * n_sp, n_sp))

    right, left = at_place(1), at_place(-1)
    to_right, to_left = {"sp": right, "tp": mine}, {"sp": left, "tp": mine}
    to_partner = {"sp": me, "tp": partner}

    def side(d):
        return lax.rem(x_at + d, n_x) * 2 + core

    def to_side(d):
        return {"sp": me, "tp": side(d)}

    def from_side(d):
        return lax.rem(x_at - d + n_x, n_x) * 2 + core

    barrier = pltpu.get_barrier_semaphore()
    pl.semaphore_signal(barrier, inc=1, device_id=to_right, device_id_type=MESH)
    pl.semaphore_signal(barrier, inc=1, device_id=to_left, device_id_type=MESH)
    for d in range(1, n_tp):
        peer = {"sp": me, "tp": lax.rem(mine + d, n_tp)}
        pl.semaphore_signal(barrier, inc=1, device_id=peer, device_id_type=MESH)
    pl.semaphore_wait(barrier, n_tp + 1)

    def piece(ref, i):
        return ref.at[pl.ds(pl.multiple_of(i * half, half), half), :]

    def ring_copies(e, first=False):
        hop, i = e // 2 + 1, lax.rem(e, 2)
        behind, beyond = at_place(1 - hop), at_place(hop - 1)
        return (
            remote(
                piece(wg_ref if first else gate_all.at[behind], i),
                piece(gate_all.at[behind], i),
                ring_sem.at[0, e],
                ring_sem.at[1, e],
                to_right,
            ),
            remote(
                piece(wu_ref if first else up_all.at[beyond], i),
                piece(up_all.at[beyond], i),
                ring_sem.at[2, e],
                ring_sem.at[3, e],
                to_left,
            ),
        )

    def down_copies(f, first=False):
        hop, i = f // 2 + 1, lax.rem(f, 2)
        behind, beyond = at_place(1 - hop), at_place(hop - 1)
        return (
            remote(
                piece(wd_ref if first else down_all.at[behind], i),
                piece(down_all.at[behind], i),
                down_sem.at[0, f],
                down_sem.at[1, f],
                to_right,
            ),
            remote(
                piece(wd_ref if first else down_all.at[beyond], i),
                piece(down_all.at[beyond], i),
                down_sem.at[2, f],
                down_sem.at[3, f],
                to_left,
            ),
        )

    def down_valid(f):
        last = f // 2 + 1 == forward
        inside = f // 2 + 1 <= forward
        even = lax.rem(f, 2) == 0
        ahead = jnp.logical_and(inside, jnp.logical_or(jnp.logical_not(last), even))
        back = jnp.logical_and(
            inside, jnp.logical_or(jnp.logical_not(last), jnp.logical_not(even))
        )
        return ahead, back

    def down_event(f):
        for copy, valid in zip(down_copies(f), down_valid(f)):

            @pl.when(valid)
            def _():
                copy.wait_recv()

        for way, valid in enumerate(down_valid(f + 2)):

            @pl.when(valid)
            def _():
                down_copies(f + 2)[way].start()

    def ring_event(e):
        for copy in ring_copies(e):
            copy.wait_recv()

        @pl.when(e + 2 < events)
        def _():
            for copy in ring_copies(e + 2):
                copy.start()

        @pl.when(e == events - 7)
        def _():
            for f in range(2):
                for copy in down_copies(jnp.int32(f), True):
                    copy.start()

    def quarter(owner, t):
        return lat_all.at[owner, pl.ds(pl.multiple_of(t * share, share), share), :]

    def lat_hop(hop, way):
        owner = at_place(jnp.where(way == 0, 1 - hop, hop - 1))
        where = {"sp": jnp.where(way == 0, right, left), "tp": mine}
        return remote(
            quarter(owner, mine),
            quarter(owner, mine),
            lat_ring.at[0, way, hop],
            lat_ring.at[1, way, hop],
            where,
        )

    def lat_owner(hop, way):
        return at_place(jnp.where(way == 0, -hop, hop))

    def lat_pair_copy(hop, way, t):
        owner = lat_owner(hop, way)
        return remote(
            quarter(owner, t),
            quarter(owner, t),
            lat_pair.at[0, way, hop],
            lat_pair.at[1, way, hop],
            to_partner,
        )

    def lat_side_copy(hop, way, d, t):
        owner = lat_owner(hop, way)
        return remote(
            quarter(owner, t),
            quarter(owner, t),
            lat_side.at[0, way, hop, d],
            lat_side.at[1, way, hop, d],
            to_side(d),
        )

    def lat_relay_copy(hop, way, d, t):
        owner = lat_owner(hop, way)
        return remote(
            quarter(owner, t),
            quarter(owner, t),
            lat_relay.at[0, way, hop, d],
            lat_relay.at[1, way, hop, d],
            to_partner,
        )

    def ways(hop):
        return jnp.where(hop <= backward, 2, 1)

    def lat_forward(hop):
        def one(way, carry):
            lat_hop(hop, way).wait_recv()

            @pl.when(hop + 1 <= jnp.where(way == 0, forward, backward))
            def _():
                lat_hop(hop + 1, way).start()

            for d in range(1, n_x):
                lat_side_copy(hop, way, d, mine).start()
            lat_pair_copy(hop, way, mine).start()
            return carry

        lax.fori_loop(0, ways(hop), one, 0)

    def lat_pass(hop):
        def one(way, carry):
            for d in range(1, n_x):
                lat_side_copy(hop, way, d, from_side(d)).wait_recv()
                lat_relay_copy(hop, way, d, from_side(d)).start()
            return carry

        lax.fori_loop(0, ways(hop), one, 0)

    def lat_ready(hop, way):
        lat_pair_copy(hop, way, partner).wait_recv()
        for d in range(1, n_x):
            lat_relay_copy(hop, way, d, from_side(d) + 1 - 2 * core).wait_recv()

    def wo_copy(kind, d, t, src=None):
        where = to_partner if kind != 1 else to_side(d)
        return remote(
            wo_all.at[t] if src is None else src,
            wo_all.at[t],
            wo_sem.at[0, kind, d],
            wo_sem.at[1, kind, d],
            where,
        )

    def rotated(values, span):
        first = first_row + span
        position = (first + lax.broadcasted_iota(jnp.int32, values.shape, 0)).astype(F32)
        angle = position * freq_ref[...]
        front = lax.rem(lax.broadcasted_iota(jnp.int32, values.shape, 1), ROPE) < ROPE // 2
        return angle, front

    def turn(values, cosine, sine, front):
        other = jnp.where(
            front,
            pltpu.roll(values, LANES - ROPE // 2, 1),
            pltpu.roll(values, ROPE // 2, 1),
        )
        return values * cosine + other * sine

    first_row = me * rows

    def prepare(i, carry):
        start = pl.multiple_of(i * share, share)
        span = pl.ds(start, share)
        key = kr_ref[span, :].astype(F32)
        key = jnp.concatenate([key, key], axis=1)
        angle, front = rotated(key, start)
        cosine = jnp.cos(angle)
        sine = jnp.sin(angle)
        sine = jnp.where(front, -sine, sine)
        lat_all[me, span, rank:] = turn(key, cosine, sine, front).astype(BF16)
        latent = lat_ref[span, :].astype(F32)
        power = jnp.mean(latent * latent, axis=1, keepdims=True)
        latent = latent * lax.rsqrt(power + norm_eps) * gain_ref[...]
        lat_all[me, span, :rank] = latent.astype(BF16)
        for j in range(heads // 2):
            pair = qr_ref[span, j * LANES : (j + 1) * LANES].astype(F32)
            pair = turn(pair, cosine, sine, front)
            q_s[2 * j, span, NOPE:] = pair.astype(BF16)
            q_s[2 * j + 1, span, NOPE:] = pltpu.roll(pair, ROPE, 1).astype(BF16)
        for h in range(heads):
            q_s[h, span, :NOPE] = qn_ref[span, h * NOPE : (h + 1) * NOPE]
        return carry

    for copy in ring_copies(jnp.int32(0), True):
        copy.start()
    for h in range(heads):
        wb_s[h, :, :NOPE] = wk_ref[:, h * NOPE : (h + 1) * NOPE]
        wb_s[h, :, NOPE:] = wv_ref[:, h * VDIM : (h + 1) * VDIM]
    lax.fori_loop(0, n_tp, prepare, 0)
    lat_hop(1, jnp.int32(0)).start()
    if backward:
        lat_hop(1, jnp.int32(1)).start()
    for copy in ring_copies(jnp.int32(1), True):
        copy.start()

    tiles = rows // tile
    chunks = rows // chunk
    total = heads * tiles
    scale = (NOPE + ROPE) ** (-0.5) * LOG2E

    m_s[...] = jnp.full_like(m_s, masked_score)
    acc_s[...] = jnp.zeros_like(acc_s)
    for h in range(heads):
        v_s[h, VDIM:, :] = jnp.ones((ONES, rows), BF16)

    def project(owner):
        def one(h, carry):
            both = jnp.dot(
                lat_all[owner, :, :rank], wb_s[h], preferred_element_type=F32
            ).astype(BF16)
            k_s[h, :, :NOPE] = both[:, :NOPE]
            k_s[h, :, NOPE:] = lat_all[owner, :, rank:]
            v_s[h, :VDIM, :] = both[:, NOPE:].T
            return carry

        lax.fori_loop(0, heads, one, 0)

    def span_of(t):
        return pl.ds(t * tile if isinstance(t, int) else pl.multiple_of(t * tile, tile), tile)

    def score(h, t, c, slot, top, diagonal):
        keys = slice(c * chunk, (c + 1) * chunk)
        scores = scale * lax.dot_general(
            k_s[h, keys, : NOPE + ROPE],
            q_s[h, span_of(t), : NOPE + ROPE],
            COLS,
            preferred_element_type=F32,
        )
        if diagonal:
            row = t * tile + lax.broadcasted_iota(jnp.int32, scores.shape, 1)
            col = c * chunk + lax.broadcasted_iota(jnp.int32, scores.shape, 0)
            scores = jnp.where(col <= row, scores, masked_score)
        s_s[slot, keys, :] = scores
        peak = jnp.max(scores.reshape(chunk // 8, 8, tile), axis=0)
        return peak if top is None else jnp.maximum(top, peak)

    def advance(h, t, peak):
        old = m_s[h, :, span_of(t)]
        top = jnp.maximum(old, jnp.max(peak, axis=0, keepdims=True))
        m_s[h, :, span_of(t)] = top
        return top[:1], jnp.exp2(old - top)[:1]

    def fold(h, c, slot, top, mixed):
        keys = slice(c * chunk, (c + 1) * chunk)
        weights = jnp.exp2(s_s[slot, keys, :] - top).astype(BF16)
        term = jnp.dot(v_s[h, :, keys], weights, preferred_element_type=F32)
        return term if mixed is None else mixed + term

    def finish(h, t, factor, mixed):
        acc_s[h, :, span_of(t)] = acc_s[h, :, span_of(t)] * factor + mixed

    project(me)

    def own_head(h, carry):
        for t in range(tiles):
            peak = mixed = None
            limit = -(-(t + 1) * tile // chunk)
            for c in range(limit):
                peak = score(h, t, c, t % 2, peak, (c + 1) * chunk > t * tile)
            top, factor = advance(h, t, peak)
            for c in range(limit):
                mixed = fold(h, c, t % 2, top, mixed)
            finish(h, t, factor, mixed)
        return carry

    lax.fori_loop(0, heads, own_head, 0)

    def attend(owner):
        project(owner)
        peak = None
        for c in range(chunks):
            peak = score(0, 0, c, 0, peak, False)
        mx_s[0] = peak

        def one(i, slot):
            h, t = i // tiles, lax.rem(i, tiles)
            later = jnp.minimum(i + 1, total - 1)
            next_h, next_t = later // tiles, lax.rem(later, tiles)
            top, factor = advance(h, t, mx_s[slot])
            peak = mixed = None
            for c in range(chunks):
                peak = score(next_h, next_t, c, 1 - slot, peak, False)
                mixed = fold(h, c, slot, top, mixed)
            mx_s[1 - slot] = peak
            finish(h, t, factor, mixed)

        def two(i, carry):
            one(2 * i, 0)
            one(2 * i + 1, 1)
            return carry

        lax.fori_loop(0, total // 2, two, 0)

    lat_forward(jnp.int32(1))
    lat_pass(jnp.int32(1))

    def block(i, carry):
        hop = i // 2 + 1
        way = lax.rem(i, 2)

        @pl.when(way < ways(hop))
        def _():
            lat_ready(hop, way)
            owner = lat_owner(hop, way)

            @pl.when(owner < me)
            def _():
                attend(owner)

        @pl.when(jnp.logical_and(way == 0, hop < forward))
        def _():
            lat_forward(hop + 1)

        @pl.when(i == 2 * forward - 4)
        def _():
            for d in range(1, n_x):
                wo_copy(1, d, mine, wo_ref).start()
            wo_copy(0, 0, mine, wo_ref).start()

        @pl.when(jnp.logical_and(way == 1, hop < forward))
        def _():
            lat_pass(hop + 1)

        ring_event(i)
        return carry

    lax.fori_loop(0, 2 * forward, block, 0)
    serviced = 2 * forward

    def finish_head(h):
        done = acc_s[h]
        out = (done[:VDIM] / done[VDIM : VDIM + 1]).T.astype(BF16)
        for r in range(n_tp):
            ho_s[r, :, h * VDIM : (h + 1) * VDIM] = out[r * share : (r + 1) * share]

    for h in range(heads):
        finish_head(h)
    tr_s[mine] = ho_s[mine]

    def trade(d):
        target = lax.rem(mine + d, n_tp)
        return remote(
            ho_s.at[target],
            tr_s.at[mine],
            trade_sem.at[0, d],
            trade_sem.at[1, d],
            {"sp": me, "tp": target},
        )

    def traded(d):
        source = lax.rem(mine - d + n_tp, n_tp)
        return remote(
            ho_s.at[source],
            tr_s.at[source],
            trade_sem.at[0, d],
            trade_sem.at[1, d],
            {"sp": me, "tp": source},
        )

    for d in range(1, n_tp):
        trade(d).start()
    for d in range(1, n_x):
        wo_copy(1, d, from_side(d)).wait_recv()
        wo_copy(2, d, from_side(d)).start()
    wo_copy(0, 0, partner).wait_recv()
    for d in range(1, n_x):
        wo_copy(2, d, from_side(d) + 1 - 2 * core).wait_recv()

    wide = wo_s.shape[3]
    columns = depth // wide

    def wo_loads(j):
        span = pl.ds(j * wide, wide)
        own = pltpu.make_async_copy(
            wo_ref.at[:, span], wo_s.at[j % 2, 0], wo_local.at[0, j % 2]
        )
        others = [
            pltpu.make_async_copy(
                wo_all.at[lax.rem(mine + d, n_tp), :, span],
                wo_s.at[j % 2, d],
                wo_local.at[d, j % 2],
            )
            for d in range(1, n_tp)
        ]
        return [own] + others

    for copy in wo_loads(0):
        copy.start()
    for d in range(1, n_tp):
        traded(d).wait_recv()
    for j in range(columns):
        for copy in wo_loads(j):
            copy.wait()
        if j + 1 < columns:
            for copy in wo_loads(j + 1):
                copy.start()
        proj = resid_ref[:, j * wide : (j + 1) * wide].astype(F32)
        for d in range(n_tp):
            group = lax.rem(mine + d, n_tp)
            proj += jnp.dot(tr_s[group], wo_s[j % 2, d], preferred_element_type=F32)
        stream_s[:, j * wide : (j + 1) * wide] = proj

    strip = divisor(share, (64, 32, 16, 8))

    def normalise(i, carry):
        span = pl.ds(pl.multiple_of(i * strip, strip), strip)
        stream = stream_s[span, :]
        power = jnp.mean(stream * stream, axis=1, keepdims=True)
        x_s[mine, span, :] = (stream * lax.rsqrt(power + norm_eps) * mix_ref[...]).astype(BF16)
        return carry

    lax.fori_loop(0, share // strip, normalise, 0)

    def x_copy(kind, d, t):
        where = to_partner if kind != 1 else to_side(d)
        return remote(x_s.at[t], x_s.at[t], x_sem.at[0, kind, d], x_sem.at[1, kind, d], where)

    for d in range(1, n_x):
        x_copy(1, d, mine).start()
    x_copy(0, 0, mine).start()
    ring_event(jnp.int32(serviced))

    def slab_copies(s, own=False):
        slot = lax.rem(s, 2) if not own else 0
        return (
            pltpu.make_async_copy(
                wg_ref if own else gate_all.at[at_place(-s)], g_buf.at[slot], local_sem.at[2, slot]
            ),
            pltpu.make_async_copy(
                wu_ref if own else up_all.at[at_place(s)], u_buf.at[slot], local_sem.at[3, slot]
            ),
        )

    def multiply(s, slot, start, last, low=0, high=n_tp):
        behind = pl.ds(pl.multiple_of(at_place(-s) * part, part), part)
        ahead = pl.ds(pl.multiple_of(at_place(s) * part, part), part)

        def one(q, carry):
            r = lax.rem(2 * x_at + q, n_tp)
            gate = jnp.dot(x_s[r, :, behind], g_buf[slot], preferred_element_type=F32)
            up = jnp.dot(x_s[r, :, ahead], u_buf[slot], preferred_element_type=F32)
            if not start:
                gate += gate_s[r]
                up += up_s[r]
            if last:
                hid_s[r] = (gate / (1.0 + jnp.exp(-gate)) * up).astype(BF16)
            else:
                gate_s[r] = gate
                up_s[r] = up
            return carry

        lax.fori_loop(low, high, one, 0)

    early = serviced // 2

    def early_slabs(low, high):
        for copy in slab_copies(jnp.int32(0), True):
            copy.start()
        for copy in slab_copies(jnp.int32(0), True):
            copy.wait()
        for copy in slab_copies(jnp.int32(1)):
            copy.start()
        multiply(jnp.int32(0), 0, True, False, low, high)

        def one_slab(s, carry):
            for copy in slab_copies(s):
                copy.wait()

            @pl.when(s < early)
            def _():
                for copy in slab_copies(s + 1):
                    copy.start()

            multiply(s, lax.rem(s, 2), False, False, low, high)
            return carry

        lax.fori_loop(1, early + 1, one_slab, 0)

    x_copy(0, 0, partner).wait_recv()
    early_slabs(0, 2)
    ring_event(jnp.int32(serviced + 1))
    for d in range(1, n_x):
        x_copy(1, d, from_side(d)).wait_recv()
        x_copy(2, d, from_side(d)).start()
    serviced += 2
    for _ in range(2):
        ring_event(jnp.int32(serviced))
        serviced += 1
    for d in range(1, n_x):
        x_copy(2, d, from_side(d) + 1 - 2 * core).wait_recv()
    early_slabs(2, n_tp)

    ready = serviced // 2
    for copy in slab_copies(jnp.int32(early + 1)):
        copy.start()

    def middle(s, carry):
        for copy in slab_copies(s):
            copy.wait()

        @pl.when(s >= ready)
        def _():
            ring_event(2 * s)
            ring_event(2 * s + 1)

        for copy in slab_copies(s + 1):
            copy.start()
        multiply(s, lax.rem(s, 2), False, False)
        return carry

    lax.fori_loop(early + 1, n_sp - 1, middle, 0)
    for copy in slab_copies(jnp.int32(n_sp - 1)):
        copy.wait()
    down_event(jnp.int32(0))
    down_event(jnp.int32(1))
    multiply(jnp.int32(n_sp - 1), (n_sp - 1) % 2, False, True)

    def down_load(k, own=False):
        slot = lax.rem(k, 2) if not own else 0
        hop = (k + 1) // 2
        owner = at_place(jnp.where(lax.rem(k, 2) == 1, -hop, hop))
        return pltpu.make_async_copy(
            wd_ref if own else down_all.at[owner], g_buf.at[slot], local_sem.at[2, slot]
        )

    def down_arrive(k):
        @pl.when(k > 1)
        def _():
            down_event(k - 1)
            down_event(k)

    def pair_copy(k):
        return remote(
            pair_out.at[k], pair_in.at[k], pair_sem.at[0, k], pair_sem.at[1, k], to_partner
        )

    def cross_copy(k, d):
        return remote(
            cross_out.at[k, d - 1],
            cross_in.at[k, d - 1],
            cross_sem.at[0, k, d],
            cross_sem.at[1, k, d],
            to_side(d),
        )

    def make(k):
        slot = lax.rem(k, 2)

        def one(x, carry):
            away = lax.dot_general(
                hid_s[2 * x + 1 - core], g_buf[slot], COLS, preferred_element_type=F32
            )
            pair_out[k, x] = away.astype(BF16)
            return carry

        lax.fori_loop(0, n_x, one, 0)

        def two(x, carry):
            keep_s[slot, x] = lax.dot_general(
                hid_s[2 * x + core], g_buf[slot], COLS, preferred_element_type=F32
            )
            return carry

        lax.fori_loop(0, n_x, two, 0)
        pair_copy(k).start()

    def combine(k):
        slot = lax.rem(k, 2)
        pair_copy(k).wait_recv()
        for d in range(1, n_x):
            x = lax.rem(x_at + d, n_x)
            cross_out[k, d - 1] = (keep_s[slot, x] + pair_in[k, x].astype(F32)).astype(BF16)
            cross_copy(k, d).start()
        owner = at_place(jnp.where(lax.rem(k, 2) == 1, -((k + 1) // 2), (k + 1) // 2))
        span = pl.ds(pl.multiple_of(owner * part, part), part)
        mixed = keep_s[slot, x_at] + pair_in[k, x_at].astype(F32)
        stream_s[:, span] = stream_s[:, span] + 0.5 * mixed

    def deliver(k):
        owner = at_place(jnp.where(lax.rem(k, 2) == 1, -((k + 1) // 2), (k + 1) // 2))
        span = pl.ds(pl.multiple_of(owner * part, part), part)
        total = stream_s[:, span]
        for d in range(1, n_x):
            cross_copy(k, d).wait_recv()
            total += 0.5 * cross_in[k, d - 1].astype(F32)
        o_ref[:, span] = total.astype(BF16)

    down_load(jnp.int32(0), True).start()
    down_load(jnp.int32(0), True).wait()

    def down_step(k, carry):
        @pl.when(jnp.logical_and(lax.rem(k, 2) == 1, k < n_sp))
        def _():
            down_arrive(k)
            down_load(k).start()

            @pl.when(k + 1 < n_sp)
            def _():
                down_load(k + 1).start()

        @pl.when(jnp.logical_and(k > 0, k < n_sp))
        def _():
            down_load(k).wait()

        @pl.when(k < n_sp)
        def _():
            make(k)

        @pl.when(jnp.logical_and(k > 0, k <= n_sp))
        def _():
            combine(k - 1)

        @pl.when(k > 1)
        def _():
            deliver(k - 2)

        return carry

    lax.fori_loop(0, n_sp + 2, down_step, 0)

    def sent_ring(e, carry):
        for copy in ring_copies(e):
            copy.wait_send()
        return carry

    lax.fori_loop(0, events, sent_ring, 0)

    def sent_hop(hop, carry):
        for i in range(2):
            f = 2 * (hop - 1) + i
            for copy, valid in zip(down_copies(f), down_valid(f)):

                @pl.when(valid)
                def _():
                    copy.wait_send()

        def one(way, carry):
            lat_hop(hop, way).wait_send()
            lat_pair_copy(hop, way, mine).wait_send()
            for d in range(1, n_x):
                lat_side_copy(hop, way, d, mine).wait_send()
                lat_relay_copy(hop, way, d, from_side(d)).wait_send()
            return carry

        lax.fori_loop(0, ways(hop), one, 0)
        return carry

    lax.fori_loop(1, forward + 1, sent_hop, 0)
    for kind in range(3):
        for d in range(1, n_x) if kind else range(1):
            wo_copy(kind, d, mine).wait_send()
            x_copy(kind, d, mine).wait_send()
    for d in range(1, n_tp):
        trade(d).wait_send()

    def sent_sum(k, carry):
        pair_copy(k).wait_send()
        for d in range(1, n_x):
            cross_copy(k, d).wait_send()
        return carry

    lax.fori_loop(0, n_sp, sent_sum, 0)


def layer(n_sp, n_tp, resid, qn, qr, latent, key_rope, freq, gain, mix, wk, wv, w_out, wg, wu, wd):
    rows = qr.shape[0]
    heads, rank = wk.shape[1] // NOPE, wk.shape[0]
    share, depth = resid.shape
    part, units = wg.shape
    n_x = n_tp // 2
    forward = n_sp // 2
    tile = divisor(rows, (512, 256, 128))
    chunk = divisor(rows, (512, 256, 128))
    wide = divisor(depth, (256, 128))
    vmem = pl.BlockSpec(memory_space=pltpu.VMEM)
    anywhere = pl.BlockSpec(memory_space=pl.ANY)
    dma = pltpu.SemaphoreType.DMA
    results = pl.pallas_call(
        functools.partial(layer_kernel, n_sp, n_tp, tile, chunk),
        out_shape=(
            jax.ShapeDtypeStruct((share, depth), BF16),
            jax.ShapeDtypeStruct((n_sp, part, units), BF16),
            jax.ShapeDtypeStruct((n_sp, part, units), BF16),
            jax.ShapeDtypeStruct((n_sp, part, units), BF16),
            jax.ShapeDtypeStruct((n_tp, heads * VDIM, depth), BF16),
        ),
        in_specs=[vmem] * 10 + [anywhere] * 4,
        out_specs=(vmem, anywhere, anywhere, anywhere, anywhere),
        scratch_shapes=[
            pltpu.VMEM((n_sp, rows, rank + LANES), BF16),
            pltpu.VMEM((heads, rank, NOPE + VDIM), BF16),
            pltpu.VMEM((heads, rows, NOPE + LANES), BF16),
            pltpu.VMEM((heads, rows, NOPE + LANES), BF16),
            pltpu.VMEM((heads, VDIM + ONES, rows), BF16),
            pltpu.VMEM((heads, 8, rows), F32),
            pltpu.VMEM((heads, VDIM + ONES, rows), F32),
            pltpu.VMEM((2, rows, tile), F32),
            pltpu.VMEM((2, 8, tile), F32),
            pltpu.VMEM((n_tp, share, heads * VDIM), BF16),
            pltpu.VMEM((n_tp, share, heads * VDIM), BF16),
            pltpu.VMEM((2, n_tp, heads * VDIM, wide), BF16),
            pltpu.VMEM((n_tp, share, depth), BF16),
            pltpu.VMEM((share, depth), F32),
            pltpu.VMEM((n_tp, share, units), F32),
            pltpu.VMEM((n_tp, share, units), F32),
            pltpu.VMEM((n_tp, share, units), BF16),
            pltpu.VMEM((2, part, units), BF16),
            pltpu.VMEM((2, part, units), BF16),
            pltpu.VMEM((2, n_x, share, part), F32),
            pltpu.VMEM((n_sp, n_x, share, part), BF16),
            pltpu.VMEM((n_sp, n_x, share, part), BF16),
            pltpu.VMEM((n_sp, n_x - 1, share, part), BF16),
            pltpu.VMEM((n_sp, n_x - 1, share, part), BF16),
            dma((2, 2, forward + 1)),
            dma((2, 2, forward + 1)),
            dma((2, 2, forward + 1, n_x)),
            dma((2, 2, forward + 1, n_x)),
            dma((2, 3, n_x)),
            dma((4, 2 * (n_sp - 1))),
            dma((4, 2 * forward)),
            dma((2, n_tp)),
            dma((2, 3, n_x)),
            dma((2, n_sp)),
            dma((2, n_sp, n_x)),
            dma((4, 2)),
            dma((n_tp, 2)),
        ],
        compiler_params=pltpu.CompilerParams(
            collective_id=0, has_side_effects=True, vmem_limit_bytes=67043328
        ),
    )(resid, qn, qr, latent, key_rope, freq, gain, mix, wk, wv, w_out, wg, wu, wd)
    return results[0]


def on_device(
    n_sp,
    n_tp,
    resid,
    query_nope,
    query_rope,
    latent,
    key_rope,
    latent_gain,
    w_key,
    w_value,
    w_out,
    mix_gain,
    w_gate,
    w_up,
    w_down,
):
    half_width = ROPE // 2
    frequency = theta_base ** (-2.0 * np.arange(half_width) / ROPE)
    frequency = jnp.asarray(np.tile(frequency, LANES // half_width)[None, :], F32)
    return layer(
        n_sp,
        n_tp,
        resid,
        query_nope,
        query_rope,
        latent,
        key_rope,
        frequency,
        latent_gain[None, :],
        mix_gain[None, :],
        w_key,
        w_value,
        w_out,
        w_gate,
        w_up,
        w_down,
    )


def solution(mesh):
    return jax.shard_map(
        functools.partial(on_device, mesh.shape["sp"], mesh.shape["tp"]),
        mesh=mesh,
        in_specs=(
            P(("sp", "tp"), None),
            P("sp", "tp"),
            P("sp", "tp"),
            P("sp", None),
            P("sp", None),
            P(),
            P(None, "tp"),
            P(None, "tp"),
            P("tp", None),
            P(),
            P("sp", "tp"),
            P("sp", "tp"),
            P("sp", "tp"),
        ),
        out_specs=P(("sp", "tp"), None),
        check_vma=False,
    )
```
